256 devices in a mesh: grp: 4 (over y, x), ep: 32 (over z), tp: 2 (over core).
Axes of the slice: x: 2, y: 2, z: 32, core: 2. Of those that a mesh axis runs over, the one named last changes fastest.
The devices are a block of a 4x16x32 slice.
Arguments:
- tokens: bfloat16 [32768, 2048], P(('grp', 'ep')), parts along dimension 0, may hold values from -6 to 6
- picks: int32 [32, 4096], P(None, ('grp', 'ep')), parts along dimension 1, may hold values from 0 to 8191, as said below
- route_weights: bfloat16 [32, 4096], P(None, ('grp', 'ep')), parts along dimension 1, may hold values from 0.19921875 to 1
- gate_weight: bfloat16 [32, 2048, 1024], P('ep', None, 'tp'), may hold values from -0.125 to 0.125
- up_weight: bfloat16 [32, 2048, 1024], P('ep', None, 'tp'), may hold values from -0.125 to 0.125
- down_weight: bfloat16 [32, 1024, 2048], P('ep', 'tp'), may hold values from -0.1875 to 0.1875
Outputs:
- mixed: bfloat16 [32768, 2048], P(('grp', 'ep'), 'tp'), parts along dimension 0
The draws below stay inside these ranges and needn't reach their ends.
There are 4 independent parts, one for each index of `grp`. The reference program is written for one: setup_inputs(seed, part) draws one part's arguments, and reference() takes and returns one part's arrays. A program takes and returns all parts, laid end to end along the dimension named above; an argument that names none is the same for every part. Nothing has to cross between parts.
Inputs may be any that keep to these rules, and one draw needn't show every extreme that they name: `picks`: slots k * 32 to (k + 1) * 32 - 1 of every expert name 32 different tokens of the block k * 256 to (k + 1) * 256 - 1.
All inputs are finite; a program needn't handle non-finite values.
Results may differ from the reference program's by a relative error of at most 0.0066.
Values may be sent and summed in bfloat16 or wider, within the bound.
A program may use at most 64 MiB of HBM per device.

```python
import jax
import jax.numpy as jnp
from jax import lax

D = 2048
FF = 1024
TOK_DEV = 256
PER = 32
EXPERTS = 32
CAP = 1024
TOKENS = 8192
N_TP = 2


def draw_picks(key, part):
    sources = TOKENS // TOK_DEV
    keys = jax.random.split(jax.random.fold_in(key, 7), EXPERTS * sources)
    chosen = jax.vmap(lambda single: jax.random.permutation(single, TOK_DEV)[:PER])(keys)
    offsets = jnp.arange(sources, dtype=jnp.int32) * TOK_DEV
    chosen = chosen.astype(jnp.int32).reshape(EXPERTS, sources, PER) + offsets[None, :, None]
    return chosen.reshape(EXPERTS, sources * PER).astype(jnp.int32)


def block_levels(rng, extent, pieces, low, largest):
    level, own = 1.0, jax.random.fold_in(rng, 6)
    for axis_at, blocks in pieces:
        steps = jnp.exp(jax.random.uniform(jax.random.fold_in(own, axis_at), (blocks,), jnp.float32, low / len(pieces), largest / len(pieces)))
        level = level * jnp.repeat(steps, extent[axis_at] // blocks).reshape([-1 if axis == axis_at else 1 for axis in range(len(extent))])
    return level


def noise(rng, shape, scale, most, pieces=(), kind=jnp.bfloat16):
    loudness = block_levels(rng, shape, pieces, -0.22, 0.18) if pieces else 1.0
    array = jax.random.normal(rng, shape, jnp.float32) * scale * loudness
    return jnp.minimum(jnp.maximum(array, -most), most).astype(kind)


def setup_inputs(seed: int = 0, part: int = 0) -> dict:
    streams_of = jax.random.split(jax.random.key(seed), 7)
    part_splits = jax.random.split(jax.random.fold_in(streams_of[6], part), 7)
    tokens = noise(part_splits[0], (TOKENS, D), 1.0, 6.0, ((0, 32),))
    picks = draw_picks(jax.random.fold_in(jax.random.fold_in(streams_of[6], part), 71), part)
    route_weights = jnp.clip(0.19921875 + 0.80078125 * jax.random.uniform(part_splits[2], (EXPERTS, CAP), jnp.float32) ** block_levels(part_splits[2], (EXPERTS, CAP), ((1, 32),), -0.2, 0.2), 0.19921875, 1.0).astype(jnp.bfloat16)
    gate_weight = noise(streams_of[3], (EXPERTS, D, FF), D ** -0.5, 0.125, ((0, 32), (2, 2)))
    up_weight = noise(streams_of[4], (EXPERTS, D, FF), D ** -0.5, 0.125, ((0, 32), (2, 2)))
    down_weight = noise(streams_of[5], (EXPERTS, FF, D), FF ** -0.5, 0.1875, ((0, 32), (1, 2)))
    return dict(tokens=tokens, picks=picks, route_weights=route_weights, gate_weight=gate_weight, up_weight=up_weight, down_weight=down_weight)


def reference(tokens, picks, route_weights, gate_weight, up_weight, down_weight):
    half_width = FF // N_TP

    def one_expert(total, index):
        rows = jnp.take(tokens, picks[index], axis=0)
        gate = jnp.dot(rows, gate_weight[index], preferred_element_type=jnp.float32)
        up = jnp.dot(rows, up_weight[index], preferred_element_type=jnp.float32)
        scale = route_weights[index].astype(jnp.float32)[:, None]
        hidden = (jax.nn.silu(gate) * up * scale).astype(jnp.bfloat16)
        summed = jnp.zeros((rows.shape[0], D), jnp.float32)
        for block in range(N_TP):
            left = hidden[:, block * half_width:(block + 1) * half_width]
            right = down_weight[index, block * half_width:(block + 1) * half_width]
            partial_value = jnp.dot(left, right, preferred_element_type=jnp.float32).astype(jnp.bfloat16)
            summed = summed + partial_value.astype(jnp.float32)
        result = summed.astype(jnp.bfloat16).astype(jnp.float32)
        return total.at[picks[index]].add(result), None

    start = jnp.zeros((TOKENS, D), jnp.float32)
    total, _ = lax.scan(one_expert, start, jnp.arange(EXPERTS, dtype=jnp.int32))
    return total.astype(jnp.bfloat16)
```

```python
import functools

import jax
import jax.numpy as jnp
from jax import lax
from jax.experimental import pallas as pl
from jax.experimental.pallas import tpu as pltpu
from jax.sharding import PartitionSpec as P

F32 = jnp.float32
BF16 = jnp.bfloat16
LANES = 128
HALF_LANES = 64


def dot(a, b):
    return lax.dot_general(a, b, (((1,), (0,)), ((), ())), preferred_element_type=F32)


def dot_nt(a, b):
    return lax.dot_general(a, b, (((1,), (1,)), ((), ())), preferred_element_type=F32)


def iota(shape, dim):
    return lax.broadcasted_iota(jnp.int32, shape, dim)


def fiota(shape, dim):
    return iota(shape, dim).astype(F32)


def ones_where(cond):
    return jnp.where(cond, 1.0, 0.0)


def kernel_body(
    n, tok_dev, per, dh, ff,
    tok_hbm, picks_ref, rw_ref, wg_hbm, wu_hbm, wd_hbm, out_ref,
    tok, wg, wu, wd, buf_l, buf_s, met_l, met_s, acc_l, acc_s, x, res, pin, pout, pw_l, pw_s, pw_own,
    back_l, back_s, load_sem, sd_l, rd_l, sd_s, rd_s, sm, rm, sx, rx, sp, rp, sc_l, rc_l, sc_s, rc_s,
):
    hops = n // 2
    dense = tok_dev // per
    big = 2 * per
    z = lax.axis_index("ep")
    t = lax.axis_index("tp")
    sign = 1 - 2 * t
    ahead = (lax.rem(z + sign + n, n), lax.rem(z - sign + n, n))
    behind = (ahead[1], ahead[0])
    buf, met, acc = (buf_l, buf_s), (met_l, met_s), (acc_l, acc_s)
    pw, back = (pw_l, pw_s), (back_l, back_s)
    sd, rd, sc, rc = (sd_l, sd_s), (rd_l, rd_s), (sc_l, sc_s), (rc_l, rc_s)

    def remote(src, dst, s, r, where):
        return pltpu.make_async_remote_copy(
            src_ref=src, dst_ref=dst, send_sem=s, recv_sem=r,
            device_id=where, device_id_type=pl.DeviceIdType.MESH,
        )

    def chunks(m):
        return (big, tok_dev // big) if m > dense else (per, m)

    def rows_of(m):
        return min(tok_dev, per * m)

    def span(c, rows):
        return pl.ds(c * rows, rows)

    def token_copy(d, k, c, rows):
        at = span(c, rows)
        return remote(
            buf[d].at[k, at], buf[d].at[k + 1, at], sd[d].at[k, c], rd[d].at[k + 1, c], {"ep": ahead[d]}
        )

    def token_arrival(d, k, c, rows):
        at = span(c, rows)
        return remote(buf[d].at[k, at], buf[d].at[k, at], sd[d].at[k, c], rd[d].at[k, c], {"ep": ahead[d]})

    def meta_copy(d, k):
        return remote(met[d].at[k], met[d].at[k + 1], sm.at[d, k], rm.at[d, k + 1], {"ep": ahead[d]})

    def meta_arrival(d, k):
        return remote(met[d].at[k], met[d].at[k], sm.at[d, k], rm.at[d, k], {"ep": ahead[d]})

    def sum_copy(d, k, c, rows):
        at = span(c, rows)
        return remote(
            acc[d].at[k, at], acc[d].at[k - 1, at], sc[d].at[k, c], rc[d].at[k - 1, c], {"ep": behind[d]}
        )

    def sum_arrival(d, k, c, rows):
        at = span(c, rows)
        return remote(acc[d].at[k, at], acc[d].at[k, at], sc[d].at[k, c], rc[d].at[k, c], {"ep": behind[d]})

    def slot_rows(slot):
        return pl.ds(slot * per, per)

    def row_copy(slot, part):
        at = x.at[part, slot_rows(slot)]
        return remote(at, at, sx.at[slot], rx.at[slot], {"tp": 1 - t})

    def part_copy(i, r0, rows):
        at = pl.ds(r0, rows)
        return remote(pout.at[at], pin.at[at], sp.at[i], rp.at[i], {"tp": 1 - t})

    def slot_of(d, k):
        return 2 * k - 1 + t if d == 0 else 2 * k - t

    barrier = pltpu.get_barrier_semaphore()
    for where in ({"ep": ahead[0]}, {"ep": ahead[1]}, {"tp": 1 - t}):
        pl.semaphore_signal(barrier, inc=1, device_id=where, device_id_type=pl.DeviceIdType.MESH)
    my_half = pl.ds(pl.multiple_of(t * dh, dh), dh)
    its_half = pl.ds(pl.multiple_of((1 - t) * dh, dh), dh)
    loads = [
        pltpu.make_async_copy(tok_hbm.at[:, my_half], tok, load_sem.at[0]),
        pltpu.make_async_copy(wg_hbm.at[0], wg, load_sem.at[1]),
        pltpu.make_async_copy(wu_hbm.at[0], wu, load_sem.at[2]),
        pltpu.make_async_copy(wd_hbm.at[0], wd, load_sem.at[3]),
    ]
    for copy in loads:
        copy.start()

    ids = (picks_ref[...] - z * tok_dev).astype(F32).astype(BF16)
    eye = ones_where(iota((per, per), 0) == iota((per, per), 1)).astype(BF16)
    ids_t = dot_nt(eye, ids)
    spread = ones_where(iota((n, LANES), 1) == iota((n, LANES), 0) + n).astype(BF16)
    weights_t = dot(dot_nt(eye, rw_ref[...]).astype(BF16), spread)
    lane_e = iota((per, n), 1)
    lane_t = fiota((per, tok_dev), 1)
    meta_lane = iota((per, LANES), 1)

    def chosen_by(e):
        column = jnp.sum(jnp.where(lane_e == e, ids_t, 0.0), axis=1, keepdims=True)
        return column == lane_t

    def reach(e, far):
        member = jnp.max(ones_where(chosen_by(e)), axis=0, keepdims=True)
        d_long = lax.rem((e - z) * sign + n, n)
        d_short = lax.rem(n - d_long, n)
        d_long = jnp.where(d_long <= hops, d_long, 0).astype(F32)
        d_short = jnp.where(d_short < hops, d_short, 0).astype(F32)
        return jnp.maximum(far[0], member * d_long), jnp.maximum(far[1], member * d_short)

    zero_row = jnp.zeros((1, tok_dev), F32)
    far = lax.fori_loop(0, n, reach, (zero_row, zero_row))
    eye_t = ones_where(iota((tok_dev, tok_dev), 0) == iota((tok_dev, tok_dev), 1)).astype(BF16)
    sub_t = fiota((tok_dev, tok_dev), 0)
    lane_tt = fiota((tok_dev, tok_dev), 1)
    orders = []
    for d in (0, 1):
        wide = jnp.broadcast_to(far[d], (LANES, tok_dev)).astype(BF16)
        column = dot_nt(eye_t, wide)[:, :1]
        key_row = far[d] * tok_dev - fiota((1, tok_dev), 1)
        key_col = column * tok_dev - fiota((tok_dev, 1), 0)
        place_row = jnp.sum(ones_where(key_col > key_row), axis=0, keepdims=True)
        place_col = jnp.sum(ones_where(key_row > key_col), axis=1, keepdims=True)
        orders.append(place_row)
        back[d][...] = ones_where(place_col == lane_tt).astype(BF16)

    def place_ids(e, tiles):
        picked = chosen_by(e)
        out = []
        for d in (0, 1):
            column = jnp.sum(jnp.where(picked, orders[d], 0.0), axis=1, keepdims=True)
            out.append(tiles[d] + jnp.where(meta_lane == e, column, 0.0))
        return tuple(out)

    tiles = lax.fori_loop(0, n, place_ids, (weights_t, weights_t))
    low = iota((per // 2, LANES), 1) < HALF_LANES
    for d in (0, 1):
        folded = jnp.where(low, tiles[d][: per // 2], pltpu.roll(tiles[d][per // 2 :], HALF_LANES, axis=1))
        met[d][0] = folded.astype(BF16)
    loads[0].wait()
    for d in (0, 1):
        swap = ones_where(orders[d] == sub_t).astype(BF16)
        buf[d][0] = dot(swap, tok[...]).astype(BF16)

    pl.semaphore_wait(barrier, 3)
    for d in (0, 1):
        meta_copy(d, 0).start()
    for c in range(tok_dev // big):
        for d in (0, 1):
            token_copy(d, 0, c, big).start()

    def pick_rows(id_col, weight_col, block, slot, store_back, rows):
        gather = ones_where(id_col == fiota((per, rows), 1)).astype(BF16)
        x[t, slot_rows(slot), :] = dot(gather, block).astype(BF16)
        row_copy(slot, t).start()
        square = iota((per, per), 0) == iota((per, per), 1)
        id_row = jnp.sum(jnp.where(square, id_col, 0.0), axis=0, keepdims=True)
        weight_row = jnp.sum(jnp.where(square, weight_col, 0.0), axis=0, keepdims=True)
        store_back(jnp.where(fiota((rows, per), 0) == id_row, weight_row, 0.0).astype(BF16))

    def own_rows():
        id_col = jnp.sum(jnp.where(lane_e == z, ids_t, 0.0), axis=1, keepdims=True)
        weight_col = jnp.sum(jnp.where(meta_lane == z + n, weights_t, 0.0), axis=1, keepdims=True)

        def store(value):
            pw_own[...] = value

        pick_rows(id_col, weight_col, tok[...], 0, store, tok_dev)

    def arrived_rows(d, k, rows):
        tile = met[d][k].astype(F32)
        lane = iota((per // 2, LANES), 1)

        def column(at):
            parts = [
                jnp.sum(jnp.where(lane == at + part, tile, 0.0), axis=1, keepdims=True)
                for part in (0, HALF_LANES)
            ]
            return jnp.concatenate(parts, axis=0)

        def store(value):
            pw[d][k, :rows] = value

        slot = slot_of(d, k)
        if not isinstance(k, int):
            pass
        elif k == hops:
            slot = n - 1
        pick_rows(column(z), column(z + n), buf[d][k, :rows], slot, store, rows)

    def token_step(q, m, both):
        pairs = ((0, q), (1, q - 1)) if both else ((0, q),)
        for d, k in pairs:
            meta_arrival(d, k).wait_recv()
            if m > 1:
                meta_copy(d, k).start()
        rows_in, n_in = chunks(m)
        rows_out, n_out = chunks(m - 1)
        each = rows_in // rows_out
        for c in range(n_in):
            for d, k in pairs:
                token_arrival(d, k, c, rows_in).wait_recv()
                for piece in range(c * each, (c + 1) * each):
                    if piece < n_out:
                        token_copy(d, k, piece, rows_out).start()
        for d, k in pairs:
            arrived_rows(d, k, rows_of(m))

    fc = min(ff, 256)
    dc = min(dh, 512)

    def feed_forward(i, first, last):
        r0, rows = first * per, (last - first) * per

        @pl.loop(first, last)
        def _(slot):
            row_copy(slot, 1 - t).wait_recv()

        at = pl.ds(r0, rows)
        hidden = []
        for f in range(0, ff, fc):
            cols = pl.ds(f, fc)
            gate = dot(x[0, at, :], wg[:dh, cols]) + dot(x[1, at, :], wg[dh:, cols])
            up = dot(x[0, at, :], wu[:dh, cols]) + dot(x[1, at, :], wu[dh:, cols])
            hidden.append((gate / (1.0 + jnp.exp(-gate)) * up).astype(BF16))
        hidden = jnp.concatenate(hidden, axis=1)
        pout[at, :] = dot(hidden, wd[:, its_half]).astype(BF16)
        part_copy(i, r0, rows).start()
        mine = dot(hidden, wd[:, my_half]).astype(BF16).astype(F32)
        part_copy(i, r0, rows).wait_recv()
        res[at, :] = (mine + pin[at, :].astype(F32)).astype(BF16)

    own_rows()
    for copy in loads[1:]:
        copy.wait()
    token_step(1, hops, False)
    last_uniform = hops - dense - 1
    quarter = n // 4
    bounds = [0, quarter + 1, 2 * quarter + 1, 3 * quarter + 1, n]

    def uniform_steps(first, last):
        if last >= first:

            @pl.loop(first, last + 1)
            def _(q):
                token_step(q, hops, True)

    ready = [(bounds[i + 1] - 1) // 2 + 2 for i in range(3)]
    q = 2
    for i in range(4):
        until = hops if i == 3 else ready[i]
        stop = min(until, last_uniform)
        uniform_steps(q, stop)
        q = max(q, stop + 1)
        while q <= until:
            token_step(q, hops + 1 - q, True)
            q += 1
        feed_forward(i, bounds[i], bounds[i + 1])

    def add_to(d, k, slot, at):
        return dot(pw[d][k, at], res[slot_rows(slot), :])

    def sum_step(q, m, both):
        pairs = ((0, q), (1, q - 1)) if both else ((0, q),)
        rows_out, n_out = chunks(m)
        rows_in, n_in = chunks(m - 1)
        each = rows_out // rows_in
        order = [n_out - 1] + list(range(n_out - 1)) if m <= dense else list(range(n_out))
        for c in order:
            for d, k in pairs:
                slot = slot_of(d, k)
                if isinstance(k, int) and k == hops:
                    slot = n - 1
                at = span(c, rows_out)
                value = add_to(d, k, slot, at)
                if c * each < n_in:
                    for piece in range(c * each, (c + 1) * each):
                        sum_arrival(d, k, piece, rows_in).wait_recv()
                    value = value + acc[d][k, at].astype(F32)
                acc[d][k, at] = value.astype(BF16)
                sum_copy(d, k, c, rows_out).start()

    q = hops
    while q > 1:
        m = hops + 1 - q
        if m > dense + 1:

            @pl.loop(0, q - 1)
            def _(i):
                sum_step(q - i, m, True)

            break
        sum_step(q, m, True)
        q -= 1
    sum_step(1, hops, False)

    for d in (0, 1):
        for k in range(hops - d):
            m = hops - k - d
            rows, count = chunks(m)
            for c in range(count):
                token_copy(d, k, c, rows).wait_send()
                sum_copy(d, k + 1, c, rows).wait_send()
            meta_copy(d, k).wait_send()

    @pl.loop(0, n)
    def _(slot):
        row_copy(slot, t).wait_send()

    for i in range(4):
        part_copy(i, bounds[i] * per, (bounds[i + 1] - bounds[i]) * per).wait_send()

    total = dot(pw_own[...], res[slot_rows(0), :])
    for d in (1, 0):
        for c in range(tok_dev // big):
            sum_arrival(d, 0, c, big).wait_recv()
        total = total + dot(back[d][...], acc[d][0])
    out_ref[...] = total.astype(BF16)


def per_device(tokens, picks, route_weights, gate_weight, up_weight, down_weight):
    n = lax.axis_size("ep")
    tok_dev, width = tokens.shape
    per = picks.shape[1]
    ff = down_weight.shape[1]
    dh = width // lax.axis_size("tp")
    hops = n // 2
    most = tok_dev // per
    dma = pltpu.SemaphoreType.DMA
    vmem = pltpu.VMEM
    kernel = pl.pallas_call(
        functools.partial(kernel_body, n, tok_dev, per, dh, ff),
        out_shape=jax.ShapeDtypeStruct((tok_dev, dh), BF16),
        in_specs=[
            pl.BlockSpec(memory_space=pl.ANY),
            pl.BlockSpec(memory_space=vmem),
            pl.BlockSpec(memory_space=vmem),
            pl.BlockSpec(memory_space=pl.ANY),
            pl.BlockSpec(memory_space=pl.ANY),
            pl.BlockSpec(memory_space=pl.ANY),
        ],
        out_specs=pl.BlockSpec(memory_space=vmem),
        scratch_shapes=[
            vmem((tok_dev, dh), BF16),
            vmem((width, ff), BF16),
            vmem((width, ff), BF16),
            vmem((ff, width), BF16),
            vmem((hops + 1, tok_dev, dh), BF16),
            vmem((hops, tok_dev, dh), BF16),
            vmem((hops + 1, per // 2, LANES), BF16),
            vmem((hops, per // 2, LANES), BF16),
            vmem((hops + 1, tok_dev, dh), BF16),
            vmem((hops, tok_dev, dh), BF16),
            vmem((2, n * per, dh), BF16),
            vmem((n * per, dh), BF16),
            vmem((n * per, dh), BF16),
            vmem((n * per, dh), BF16),
            vmem((hops + 1, tok_dev, per), BF16),
            vmem((hops, tok_dev, per), BF16),
            vmem((tok_dev, per), BF16),
            vmem((tok_dev, tok_dev), BF16),
            vmem((tok_dev, tok_dev), BF16),
            dma((4,)),
            dma((hops + 1, most)), dma((hops + 1, most)), dma((hops, most)), dma((hops, most)),
            dma((2, hops + 1)), dma((2, hops + 1)),
            dma((n,)), dma((n,)),
            dma((4,)), dma((4,)),
            dma((hops + 1, most)), dma((hops + 1, most)), dma((hops, most)), dma((hops, most)),
        ],
        compiler_params=pltpu.CompilerParams(
            collective_id=0, has_side_effects=True, vmem_limit_bytes=67043328
        ),
    )
    return kernel(tokens, picks, route_weights, gate_weight, up_weight, down_weight)


def solution(mesh):
    return jax.shard_map(
        per_device,
        mesh=mesh,
        in_specs=(
            P(("grp", "ep"), None),
            P(None, ("grp", "ep")),
            P(None, ("grp", "ep")),
            P("ep", None, "tp"),
            P("ep", None, "tp"),
            P("ep", "tp", None),
        ),
        out_specs=P(("grp", "ep"), "tp"),
        check_vma=False,
    )
```

```python
import functools

import jax
import jax.numpy as jnp
from jax import lax
from jax.experimental import pallas as pl
from jax.experimental.pallas import tpu as pltpu
from jax.sharding import PartitionSpec as P

F32 = jnp.float32
BF16 = jnp.bfloat16
LANES = 128
HALF_LANES = 64


def dot(a, b):
    return lax.dot_general(a, b, (((1,), (0,)), ((), ())), preferred_element_type=F32)


def dot_nt(a, b):
    return lax.dot_general(a, b, (((1,), (1,)), ((), ())), preferred_element_type=F32)


def iota(shape, dim):
    return lax.broadcasted_iota(jnp.int32, shape, dim)


def fiota(shape, dim):
    return iota(shape, dim).astype(F32)


def ones_where(cond):
    return jnp.where(cond, 1.0, 0.0)


def kernel_body(
    n, tok_dev, per, dh, ff,
    tok_hbm, picks_ref, rw_ref, wg_hbm, wu_hbm, wd_hbm, out_ref,
    tok, wg, wu, wd, buf_l, buf_s, met_l, met_s, acc_l, acc_s, x, res, pin, pout, pw_l, pw_s, pw_own, scale,
    back_l, back_s, load_sem, sd_l, rd_l, sd_s, rd_s, sm, rm, sx, rx, sp, rp, sc_l, rc_l, sc_s, rc_s,
):
    hops = n // 2
    dense = tok_dev // per
    big = 2 * per
    z = lax.axis_index("ep")
    t = lax.axis_index("tp")
    sign = 1 - 2 * t
    ahead = (lax.rem(z + sign + n, n), lax.rem(z - sign + n, n))
    behind = (ahead[1], ahead[0])
    buf, met, acc = (buf_l, buf_s), (met_l, met_s), (acc_l, acc_s)
    pw, back = (pw_l, pw_s), (back_l, back_s)
    sd, rd, sc, rc = (sd_l, sd_s), (rd_l, rd_s), (sc_l, sc_s), (rc_l, rc_s)

    def remote(src, dst, s, r, where):
        return pltpu.make_async_remote_copy(
            src_ref=src, dst_ref=dst, send_sem=s, recv_sem=r,
            device_id=where, device_id_type=pl.DeviceIdType.MESH,
        )

    def chunks(m):
        return (big, tok_dev // big) if m > dense else (per, m)

    def rows_of(m):
        return min(tok_dev, per * m)

    def pieces(m, part):
        return range(part * (dense // 2), min(m, (part + 1) * (dense // 2)))

    def span(c, rows):
        return pl.ds(c * rows, rows)

    def token_copy(d, k, c):
        at = span(c, per)
        return remote(
            buf[d].at[k, at], buf[d].at[k + 1, at], sd[d].at[k, c], rd[d].at[k + 1, c], {"ep": ahead[d]}
        )

    def token_arrival(d, k, c):
        at = span(c, per)
        return remote(buf[d].at[k, at], buf[d].at[k, at], sd[d].at[k, c], rd[d].at[k, c], {"ep": ahead[d]})

    def meta_copy(d, k):
        return remote(met[d].at[k], met[d].at[k + 1], sm.at[d, k], rm.at[d, k + 1], {"ep": ahead[d]})

    def meta_arrival(d, k):
        return remote(met[d].at[k], met[d].at[k], sm.at[d, k], rm.at[d, k], {"ep": ahead[d]})

    def sum_copy(d, k, c, rows):
        at = span(c, rows)
        return remote(
            acc[d].at[k, at], acc[d].at[k - 1, at], sc[d].at[k, c], rc[d].at[k - 1, c], {"ep": behind[d]}
        )

    def sum_arrival(d, k, c, rows):
        at = span(c, rows)
        return remote(acc[d].at[k, at], acc[d].at[k, at], sc[d].at[k, c], rc[d].at[k, c], {"ep": behind[d]})

    def slot_rows(slot):
        return pl.ds(slot * per, per)

    def row_copy(slot, part):
        at = x.at[part, slot_rows(slot)]
        return remote(at, at, sx.at[slot], rx.at[slot], {"tp": 1 - t})

    def part_copy(i, r0, rows):
        at = pl.ds(r0, rows)
        return remote(pout.at[at], pin.at[at], sp.at[i], rp.at[i], {"tp": 1 - t})

    def slot_of(d, k):
        return 2 * k - 1 + t if d == 0 else 2 * k - t

    barrier = pltpu.get_barrier_semaphore()
    for where in ({"ep": ahead[0]}, {"ep": ahead[1]}, {"tp": 1 - t}):
        pl.semaphore_signal(barrier, inc=1, device_id=where, device_id_type=pl.DeviceIdType.MESH)
    my_half = pl.ds(pl.multiple_of(t * dh, dh), dh)
    its_half = pl.ds(pl.multiple_of((1 - t) * dh, dh), dh)
    loads = [
        pltpu.make_async_copy(tok_hbm.at[:, my_half], tok, load_sem.at[0]),
        pltpu.make_async_copy(wg_hbm.at[0], wg, load_sem.at[1]),
        pltpu.make_async_copy(wu_hbm.at[0], wu, load_sem.at[2]),
        pltpu.make_async_copy(wd_hbm.at[0], wd, load_sem.at[3]),
    ]
    for copy in loads:
        copy.start()

    ids = (picks_ref[...] - z * tok_dev).astype(F32).astype(BF16)
    eye = ones_where(iota((per, per), 0) == iota((per, per), 1)).astype(BF16)
    ids_t = dot_nt(eye, ids)
    spread = ones_where(iota((n, LANES), 1) == iota((n, LANES), 0) + n).astype(BF16)
    weights_t = dot(dot_nt(eye, rw_ref[...]).astype(BF16), spread)
    lane_e = iota((per, n), 1)
    lane_t = fiota((per, tok_dev), 1)
    meta_lane = iota((per, LANES), 1)

    def chosen_by(e):
        column = jnp.sum(jnp.where(lane_e == e, ids_t, 0.0), axis=1, keepdims=True)
        return column == lane_t

    def reach(e, far):
        member = jnp.max(ones_where(chosen_by(e)), axis=0, keepdims=True)
        d_long = lax.rem((e - z) * sign + n, n)
        d_short = lax.rem(n - d_long, n)
        d_long = jnp.where(d_long <= hops, d_long, 0).astype(F32)
        d_short = jnp.where(d_short < hops, d_short, 0).astype(F32)
        return jnp.maximum(far[0], member * d_long), jnp.maximum(far[1], member * d_short)

    zero_row = jnp.zeros((1, tok_dev), F32)
    trip = min(n, 8)

    def several(step):
        def run(i, carry):
            for j in range(trip):
                carry = step(i * trip + j, carry)
            return carry

        return run

    far = lax.fori_loop(0, n // trip, several(reach), (zero_row, zero_row))
    eye_t = ones_where(iota((tok_dev, tok_dev), 0) == iota((tok_dev, tok_dev), 1)).astype(BF16)
    sub_t = fiota((tok_dev, tok_dev), 0)
    orders = []
    for d in (0, 1):
        wide = jnp.broadcast_to(far[d], (LANES, tok_dev)).astype(BF16)
        column = dot_nt(eye_t, wide)[:, :1]
        key_row = far[d] * tok_dev - fiota((1, tok_dev), 1)
        key_col = column * tok_dev - fiota((tok_dev, 1), 0)
        place_row = jnp.sum(ones_where(key_col > key_row), axis=0, keepdims=True)
        place_col = jnp.sum(ones_where(key_row > key_col), axis=1, keepdims=True)
        orders.append(place_row)
        for c in range(tok_dev // big):
            back[d][c] = ones_where(place_col == fiota((tok_dev, big), 1) + c * big).astype(BF16)

    def place_ids(e, tiles):
        picked = chosen_by(e)
        out = []
        for d in (0, 1):
            column = jnp.sum(jnp.where(picked, orders[d], 0.0), axis=1, keepdims=True)
            out.append(tiles[d] + jnp.where(meta_lane == e, column, 0.0))
        return tuple(out)

    tiles = lax.fori_loop(0, n // trip, several(place_ids), (weights_t, weights_t))
    low = iota((per // 2, LANES), 1) < HALF_LANES
    for d in (0, 1):
        folded = jnp.where(low, tiles[d][: per // 2], pltpu.roll(tiles[d][per // 2 :], HALF_LANES, axis=1))
        met[d][0] = folded.astype(BF16)
    loads[0].wait()
    for d in (0, 1):
        swap = ones_where(orders[d] == sub_t).astype(BF16)
        buf[d][0] = dot(swap, tok[...]).astype(BF16)

    pl.semaphore_wait(barrier, 3)
    for d in (0, 1):
        meta_copy(d, 0).start()

    def own_block(part):
        for c in pieces(hops, part):
            for d in (0, 1):
                token_copy(d, 0, c).start()

    own_block(0)

    def pick_rows(id_col, weight_col, block, slot, store_back, rows):
        scale[slot_rows(slot), :] = weight_col
        gather = ones_where(id_col == fiota((per, rows), 1)).astype(BF16)
        x[t, slot_rows(slot), :] = dot(gather, block).astype(BF16)
        row_copy(slot, t).start()
        square = iota((per, per), 0) == iota((per, per), 1)
        id_row = jnp.sum(jnp.where(square, id_col, 0.0), axis=0, keepdims=True)
        store_back(ones_where(fiota((rows, per), 0) == id_row).astype(BF16))

    def own_rows():
        id_col = jnp.sum(jnp.where(lane_e == z, ids_t, 0.0), axis=1, keepdims=True)
        weight_col = jnp.sum(jnp.where(meta_lane == z + n, weights_t, 0.0), axis=1, keepdims=True)

        def store(value):
            pw_own[...] = value

        pick_rows(id_col, weight_col, tok[...], 0, store, tok_dev)

    def arrived_rows(d, k, rows):
        tile = met[d][k].astype(F32)
        lane = iota((per // 2, LANES), 1)

        def column(at):
            parts = [
                jnp.sum(jnp.where(lane == at + part, tile, 0.0), axis=1, keepdims=True)
                for part in (0, HALF_LANES)
            ]
            return jnp.concatenate(parts, axis=0)

        def store(value):
            pw[d][k, :rows] = value

        slot = slot_of(d, k)
        if not isinstance(k, int):
            pass
        elif k == hops:
            slot = n - 1
        pick_rows(column(z), column(z + n), buf[d][k, :rows], slot, store, rows)

    def token_step(part, q, m, both=True):
        pairs = ((0, q), (1, q - 1)) if both else ((0, q),)
        if part == 0:
            for d, k in pairs:
                meta_arrival(d, k).wait_recv()
                if m > 1:
                    meta_copy(d, k).start()
        onward = pieces(m - 1, part)
        for c in pieces(m, part):
            for d, k in pairs:
                token_arrival(d, k, c).wait_recv()
                if c in onward:
                    token_copy(d, k, c).start()
        if part == (0 if m <= dense // 2 else 1):
            for d, k in pairs:
                arrived_rows(d, k, rows_of(m))

    fc = min(ff, 256)

    def feed_forward(i, first, last):
        r0, rows = first * per, (last - first) * per

        @pl.loop(first, last)
        def _(slot):
            row_copy(slot, 1 - t).wait_recv()

        at = pl.ds(r0, rows)
        hidden = []
        for f in range(0, ff, fc):
            cols = pl.ds(f, fc)
            gate = dot(x[0, at, :], wg[:dh, cols]) + dot(x[1, at, :], wg[dh:, cols])
            up = dot(x[0, at, :], wu[:dh, cols]) + dot(x[1, at, :], wu[dh:, cols])
            hidden.append((gate / (1.0 + jnp.exp(-gate)) * up * scale[at, :]).astype(BF16))
        hidden = jnp.concatenate(hidden, axis=1)
        pout[at, :] = dot(hidden, wd[:, its_half]).astype(BF16)
        part_copy(i, r0, rows).start()
        mine = dot(hidden, wd[:, my_half]).astype(BF16).astype(F32)
        part_copy(i, r0, rows).wait_recv()
        res[at, :] = (mine + pin[at, :].astype(F32)).astype(BF16)

    def add_to(d, k, slot, at):
        return dot(pw[d][k, at], res[slot_rows(slot), :])

    def sum_step(q, m, both):
        pairs = ((0, q), (1, q - 1)) if both else ((0, q),)
        rows_out, n_out = chunks(m)
        rows_in, n_in = chunks(m - 1)
        each = rows_out // rows_in
        order = [n_out - 1] + list(range(n_out - 1)) if m <= dense else list(range(n_out))
        for c in order:
            for d, k in pairs:
                slot = slot_of(d, k)
                if isinstance(k, int) and k == hops:
                    slot = n - 1
                at = span(c, rows_out)
                value = add_to(d, k, slot, at)
                if c * each < n_in:
                    for piece in range(c * each, (c + 1) * each):
                        sum_arrival(d, k, piece, rows_in).wait_recv()
                    value = value + acc[d][k, at].astype(F32)
                acc[d][k, at] = value.astype(BF16)
                sum_copy(d, k, c, rows_out).start()

    def experts_left(q):
        return hops + 1 - q

    bounds = [0, hops // 2 - 1, hops - 1, 3 * hops // 2 + 1, n]

    def some_experts(i):
        feed_forward(i, bounds[i], bounds[i + 1])

    def tokens_of(part, q):
        token_step(part, q, experts_left(q))

    def sums_of(q):
        sum_step(q, experts_left(q), True)

    own_rows()
    for copy in loads[1:]:
        copy.wait()
    full = hops - dense // 2
    token_step(0, 1, hops, False)

    @pl.loop(2, full + 1)
    def _(q):
        token_step(0, q, hops, True)

    own_block(1)
    for i in range(dense // 2):
        tokens_of(0, full + 1 + i)
        token_step(1, 1 + i, experts_left(1 + i), i > 0)
    some_experts(3)
    tokens_of(1, dense // 2 + 1)
    some_experts(0)

    @pl.loop(dense // 2 + 2, hops - dense + 1)
    def _(q):
        token_step(1, q, hops, True)

    tokens_of(1, hops - dense + 1)
    some_experts(1)
    back_hop = hops
    for q in range(hops - dense + 2, full + 1):
        sums_of(back_hop)
        back_hop -= 1
        tokens_of(1, q)
    some_experts(2)
    while experts_left(back_hop) <= dense + 1:
        sums_of(back_hop)
        back_hop -= 1
    rest = back_hop

    @pl.loop(0, rest - 1)
    def _(i):
        sum_step(rest - i, hops, True)

    sum_step(1, hops, False)

    for d in (0, 1):
        for k in range(hops - d):
            m = hops - k - d
            rows, count = chunks(m)
            for c in range(min(m, dense)):
                token_copy(d, k, c).wait_send()
            for c in range(count):
                sum_copy(d, k + 1, c, rows).wait_send()
            meta_copy(d, k).wait_send()

    @pl.loop(0, n)
    def _(slot):
        row_copy(slot, t).wait_send()

    for i in range(4):
        part_copy(i, bounds[i] * per, (bounds[i + 1] - bounds[i]) * per).wait_send()

    total = dot(pw_own[...], res[slot_rows(0), :])
    for d in (1, 0):
        for c in range(tok_dev // big):
            sum_arrival(d, 0, c, big).wait_recv()
            total = total + dot(back[d][c], acc[d][0, span(c, big)])
    out_ref[...] = total.astype(BF16)


def per_device(tokens, picks, route_weights, gate_weight, up_weight, down_weight):
    n = lax.axis_size("ep")
    tok_dev, width = tokens.shape
    per = picks.shape[1]
    ff = down_weight.shape[1]
    dh = width // lax.axis_size("tp")
    hops = n // 2
    most = tok_dev // per
    dma = pltpu.SemaphoreType.DMA
    vmem = pltpu.VMEM
    kernel = pl.pallas_call(
        functools.partial(kernel_body, n, tok_dev, per, dh, ff),
        out_shape=jax.ShapeDtypeStruct((tok_dev, dh), BF16),
        in_specs=[
            pl.BlockSpec(memory_space=pl.ANY),
            pl.BlockSpec(memory_space=vmem),
            pl.BlockSpec(memory_space=vmem),
            pl.BlockSpec(memory_space=pl.ANY),
            pl.BlockSpec(memory_space=pl.ANY),
            pl.BlockSpec(memory_space=pl.ANY),
        ],
        out_specs=pl.BlockSpec(memory_space=vmem),
        scratch_shapes=[
            vmem((tok_dev, dh), BF16),
            vmem((width, ff), BF16),
            vmem((width, ff), BF16),
            vmem((ff, width), BF16),
            vmem((hops + 1, tok_dev, dh), BF16),
            vmem((hops, tok_dev, dh), BF16),
            vmem((hops + 1, per // 2, LANES), BF16),
            vmem((hops, per // 2, LANES), BF16),
            vmem((hops + 1, tok_dev, dh), BF16),
            vmem((hops, tok_dev, dh), BF16),
            vmem((2, n * per, dh), BF16),
            vmem((n * per, dh), BF16),
            vmem((n * per, dh), BF16),
            vmem((n * per, dh), BF16),
            vmem((hops + 1, tok_dev, per), BF16),
            vmem((hops, tok_dev, per), BF16),
            vmem((tok_dev, per), BF16),
            vmem((n * per, 1), F32),
            vmem((tok_dev // (2 * per), tok_dev, 2 * per), BF16),
            vmem((tok_dev // (2 * per), tok_dev, 2 * per), BF16),
            dma((4,)),
            dma((hops + 1, most)), dma((hops + 1, most)), dma((hops, most)), dma((hops, most)),
            dma((2, hops + 1)), dma((2, hops + 1)),
            dma((n,)), dma((n,)),
            dma((4,)), dma((4,)),
            dma((hops + 1, most)), dma((hops + 1, most)), dma((hops, most)), dma((hops, most)),
        ],
        compiler_params=pltpu.CompilerParams(
            collective_id=0, has_side_effects=True, vmem_limit_bytes=67043328
        ),
    )
    return kernel(tokens, picks, route_weights, gate_weight, up_weight, down_weight)


def solution(mesh):
    return jax.shard_map(
        per_device,
        mesh=mesh,
        in_specs=(
            P(("grp", "ep"), None),
            P(None, ("grp", "ep")),
            P(None, ("grp", "ep")),
            P("ep", None, "tp"),
            P("ep", None, "tp"),
            P("ep", "tp", None),
        ),
        out_specs=P(("grp", "ep"), "tp"),
        check_vma=False,
    )
```

```python
import functools

import jax
import jax.numpy as jnp
from jax import lax
from jax.experimental import pallas as pl
from jax.experimental.pallas import tpu as pltpu
from jax.sharding import PartitionSpec as P

F32 = jnp.float32
BF16 = jnp.bfloat16
LANES = 128
HALF_LANES = 64


def dot(a, b):
    return lax.dot_general(a, b, (((1,), (0,)), ((), ())), preferred_element_type=F32)


def dot_nt(a, b):
    return lax.dot_general(a, b, (((1,), (1,)), ((), ())), preferred_element_type=F32)


def iota(shape, dim):
    return lax.broadcasted_iota(jnp.int32, shape, dim)


def fiota(shape, dim):
    return iota(shape, dim).astype(F32)


def ones_where(cond):
    return jnp.where(cond, 1.0, 0.0)


def kernel_body(
    n, tok_dev, per, dh, ff,
    tok_hbm, picks_ref, rw_ref, wg_hbm, wu_hbm, wd_hbm, out_ref,
    tok, wg, wu, wd, buf_l, buf_s, met_l, met_s, acc_l, acc_s, x, res, pin, pout, pw_l, pw_s, pw_own, scale,
    back_l, back_s, load_sem, sd_l, rd_l, sd_s, rd_s, sm, rm, sx, rx, sp, rp, sc_l, rc_l, sc_s, rc_s,
):
    hops = n // 2
    dense = tok_dev // per
    big = 2 * per
    z = lax.axis_index("ep")
    t = lax.axis_index("tp")
    sign = 1 - 2 * t
    ahead = (lax.rem(z + sign + n, n), lax.rem(z - sign + n, n))
    behind = (ahead[1], ahead[0])
    buf, met, acc = (buf_l, buf_s), (met_l, met_s), (acc_l, acc_s)
    pw, back = (pw_l, pw_s), (back_l, back_s)
    sd, rd, sc, rc = (sd_l, sd_s), (rd_l, rd_s), (sc_l, sc_s), (rc_l, rc_s)

    def remote(src, dst, s, r, where):
        return pltpu.make_async_remote_copy(
            src_ref=src, dst_ref=dst, send_sem=s, recv_sem=r,
            device_id=where, device_id_type=pl.DeviceIdType.MESH,
        )

    def chunks(m):
        return (big, tok_dev // big) if m > dense else (per, m)

    def rows_of(m):
        return min(tok_dev, per * m)

    def pieces(m, part):
        return range(part * (dense // 2), min(m, (part + 1) * (dense // 2)))

    def span(c, rows):
        return pl.ds(c * rows, rows)

    def token_copy(d, k, c):
        at = span(c, per)
        return remote(
            buf[d].at[k, at], buf[d].at[k + 1, at], sd[d].at[k, c], rd[d].at[k + 1, c], {"ep": ahead[d]}
        )

    def token_arrival(d, k, c):
        at = span(c, per)
        return remote(buf[d].at[k, at], buf[d].at[k, at], sd[d].at[k, c], rd[d].at[k, c], {"ep": ahead[d]})

    def meta_copy(d, k):
        return remote(met[d].at[k], met[d].at[k + 1], sm.at[d, k], rm.at[d, k + 1], {"ep": ahead[d]})

    def meta_arrival(d, k):
        return remote(met[d].at[k], met[d].at[k], sm.at[d, k], rm.at[d, k], {"ep": ahead[d]})

    def sum_copy(d, k, c, rows):
        at = span(c, rows)
        return remote(
            acc[d].at[k, at], acc[d].at[k - 1, at], sc[d].at[k, c], rc[d].at[k - 1, c], {"ep": behind[d]}
        )

    def sum_arrival(d, k, c, rows):
        at = span(c, rows)
        return remote(acc[d].at[k, at], acc[d].at[k, at], sc[d].at[k, c], rc[d].at[k, c], {"ep": behind[d]})

    def slot_rows(slot):
        return pl.ds(slot * per, per)

    def row_copy(slot, part):
        at = x.at[part, slot_rows(slot)]
        return remote(at, at, sx.at[slot], rx.at[slot], {"tp": 1 - t})

    def part_copy(i, r0, rows):
        at = pl.ds(r0, rows)
        return remote(pout.at[at], pin.at[at], sp.at[i], rp.at[i], {"tp": 1 - t})

    def slot_of(d, k):
        return 2 * k - 1 + t if d == 0 else 2 * k - t

    barrier = pltpu.get_barrier_semaphore()
    for where in ({"ep": ahead[0]}, {"ep": ahead[1]}, {"tp": 1 - t}):
        pl.semaphore_signal(barrier, inc=1, device_id=where, device_id_type=pl.DeviceIdType.MESH)
    my_half = pl.ds(pl.multiple_of(t * dh, dh), dh)
    its_half = pl.ds(pl.multiple_of((1 - t) * dh, dh), dh)
    loads = [
        pltpu.make_async_copy(tok_hbm.at[:, my_half], tok, load_sem.at[0]),
        pltpu.make_async_copy(wg_hbm.at[0], wg, load_sem.at[1]),
        pltpu.make_async_copy(wu_hbm.at[0], wu, load_sem.at[2]),
        pltpu.make_async_copy(wd_hbm.at[0], wd, load_sem.at[3]),
    ]
    for copy in loads:
        copy.start()

    ids = (picks_ref[...] - z * tok_dev).astype(F32).astype(BF16)
    eye = ones_where(iota((per, per), 0) == iota((per, per), 1)).astype(BF16)
    ids_t = dot_nt(eye, ids)
    spread = ones_where(iota((n, LANES), 1) == iota((n, LANES), 0) + n).astype(BF16)
    weights_t = dot(dot_nt(eye, rw_ref[...]).astype(BF16), spread)
    lane_e = iota((per, n), 1)
    lane_t = fiota((per, tok_dev), 1)
    meta_lane = iota((per, LANES), 1)

    def chosen_by(e):
        column = jnp.sum(jnp.where(lane_e == e, ids_t, 0.0), axis=1, keepdims=True)
        return column == lane_t

    def reach(e, far):
        member = jnp.max(ones_where(chosen_by(e)), axis=0, keepdims=True)
        d_long = lax.rem((e - z) * sign + n, n)
        d_short = lax.rem(n - d_long, n)
        d_long = jnp.where(d_long <= hops, d_long, 0).astype(F32)
        d_short = jnp.where(d_short < hops, d_short, 0).astype(F32)
        return jnp.maximum(far[0], member * d_long), jnp.maximum(far[1], member * d_short)

    zero_row = jnp.zeros((1, tok_dev), F32)
    trip = min(n, 8)

    def several(step):
        def run(i, carry):
            for j in range(trip):
                carry = step(i * trip + j, carry)
            return carry

        return run

    far = lax.fori_loop(0, n // trip, several(reach), (zero_row, zero_row))
    eye_t = ones_where(iota((tok_dev, tok_dev), 0) == iota((tok_dev, tok_dev), 1)).astype(BF16)
    sub_t = fiota((tok_dev, tok_dev), 0)
    keys, orders, swaps = [], [], []
    for d in (0, 1):
        wide = jnp.broadcast_to(far[d], (LANES, tok_dev)).astype(BF16)
        column = dot_nt(eye_t, wide)[:, :1]
        key_row = far[d] * tok_dev - fiota((1, tok_dev), 1)
        key_col = column * tok_dev - fiota((tok_dev, 1), 0)
        place_row = jnp.sum(ones_where(key_col > key_row), axis=0, keepdims=True)
        keys.append((key_row, key_col))
        orders.append(place_row)
        swaps.append(ones_where(place_row == sub_t).astype(BF16))

    def own_block(part):
        rows = tok_dev // 2
        for d in (0, 1):
            at = slice(part * rows, (part + 1) * rows)
            buf[d][0, at] = dot(swaps[d][at], tok[...]).astype(BF16)

    def send_own_block(part):
        for c in pieces(hops, part):
            for d in (0, 1):
                token_copy(d, 0, c).start()

    loads[0].wait()
    own_block(0)
    pl.semaphore_wait(barrier, 3)
    send_own_block(0)

    def place_ids(e, tiles):
        picked = chosen_by(e)
        out = []
        for d in (0, 1):
            column = jnp.sum(jnp.where(picked, orders[d], 0.0), axis=1, keepdims=True)
            out.append(tiles[d] + jnp.where(meta_lane == e, column, 0.0))
        return tuple(out)

    tiles = lax.fori_loop(0, n // trip, several(place_ids), (weights_t, weights_t))
    low = iota((per // 2, LANES), 1) < HALF_LANES
    for d in (0, 1):
        folded = jnp.where(low, tiles[d][: per // 2], pltpu.roll(tiles[d][per // 2 :], HALF_LANES, axis=1))
        met[d][0] = folded.astype(BF16)
    own_block(1)
    for d in (0, 1):
        meta_copy(d, 0).start()
        key_row, key_col = keys[d]
        place_col = jnp.sum(ones_where(key_row > key_col), axis=1, keepdims=True)
        for c in range(tok_dev // big):
            back[d][c] = ones_where(place_col == fiota((tok_dev, big), 1) + c * big).astype(BF16)

    def pick_rows(id_col, weight_col, block, slot, store_back, rows):
        scale[slot_rows(slot), :] = weight_col
        gather = ones_where(id_col == fiota((per, rows), 1)).astype(BF16)
        x[t, slot_rows(slot), :] = dot(gather, block).astype(BF16)
        row_copy(slot, t).start()
        square = iota((per, per), 0) == iota((per, per), 1)
        id_row = jnp.sum(jnp.where(square, id_col, 0.0), axis=0, keepdims=True)
        store_back(ones_where(fiota((rows, per), 0) == id_row).astype(BF16))

    def own_rows():
        id_col = jnp.sum(jnp.where(lane_e == z, ids_t, 0.0), axis=1, keepdims=True)
        weight_col = jnp.sum(jnp.where(meta_lane == z + n, weights_t, 0.0), axis=1, keepdims=True)

        def store(value):
            pw_own[...] = value

        pick_rows(id_col, weight_col, tok[...], 0, store, tok_dev)

    def arrived_rows(d, k, rows):
        tile = met[d][k].astype(F32)
        lane = iota((per // 2, LANES), 1)

        def column(at):
            parts = [
                jnp.sum(jnp.where(lane == at + part, tile, 0.0), axis=1, keepdims=True)
                for part in (0, HALF_LANES)
            ]
            return jnp.concatenate(parts, axis=0)

        def store(value):
            pw[d][k, :rows] = value

        slot = slot_of(d, k)
        if not isinstance(k, int):
            pass
        elif k == hops:
            slot = n - 1
        pick_rows(column(z), column(z + n), buf[d][k, :rows], slot, store, rows)

    def token_step(part, q, m, both=True):
        pairs = ((0, q), (1, q - 1)) if both else ((0, q),)
        onward = pieces(m - 1, part)
        for c in pieces(m, part):
            for d, k in pairs:
                token_arrival(d, k, c).wait_recv()
                if c in onward:
                    token_copy(d, k, c).start()
        if part == 0:
            for d, k in pairs:
                meta_arrival(d, k).wait_recv()
                if m > 1:
                    meta_copy(d, k).start()
        if part == (0 if m <= dense // 2 else 1):
            for d, k in pairs:
                arrived_rows(d, k, rows_of(m))

    fc = min(ff, 256)

    def feed_forward(i, first, last):
        r0, rows = first * per, (last - first) * per

        @pl.loop(first, last)
        def _(slot):
            row_copy(slot, 1 - t).wait_recv()

        at = pl.ds(r0, rows)
        hidden = []
        for f in range(0, ff, fc):
            cols = pl.ds(f, fc)
            gate = dot(x[0, at, :], wg[:dh, cols]) + dot(x[1, at, :], wg[dh:, cols])
            up = dot(x[0, at, :], wu[:dh, cols]) + dot(x[1, at, :], wu[dh:, cols])
            hidden.append((gate / (1.0 + jnp.exp(-gate)) * up * scale[at, :]).astype(BF16))
        hidden = jnp.concatenate(hidden, axis=1)
        pout[at, :] = dot(hidden, wd[:, its_half]).astype(BF16)
        part_copy(i, r0, rows).start()
        res[at, :] = dot(hidden, wd[:, my_half]).astype(BF16)

    def join_halves(i, first, last):
        r0, rows = first * per, (last - first) * per
        at = pl.ds(r0, rows)
        part_copy(i, r0, rows).wait_recv()
        res[at, :] = (res[at, :].astype(F32) + pin[at, :].astype(F32)).astype(BF16)

    def add_to(d, k, slot, at):
        return dot(pw[d][k, at], res[slot_rows(slot), :])

    def sum_step(q, m, both):
        pairs = ((0, q), (1, q - 1)) if both else ((0, q),)
        rows_out, n_out = chunks(m)
        rows_in, n_in = chunks(m - 1)
        each = rows_out // rows_in
        order = [n_out - 1] + list(range(n_out - 1)) if m <= dense else list(range(n_out))
        for c in order:
            for d, k in pairs:
                slot = slot_of(d, k)
                if isinstance(k, int) and k == hops:
                    slot = n - 1
                at = span(c, rows_out)
                value = add_to(d, k, slot, at)
                if c * each < n_in:
                    for piece in range(c * each, (c + 1) * each):
                        sum_arrival(d, k, piece, rows_in).wait_recv()
                    value = value + acc[d][k, at].astype(F32)
                acc[d][k, at] = value.astype(BF16)
                sum_copy(d, k, c, rows_out).start()

    def experts_left(q):
        return hops + 1 - q

    bounds = [0, hops // 2 - 1, hops - 1, 5 * hops // 4 + 1, 3 * hops // 2 + 1, n]

    def some_experts(i):
        feed_forward(i, bounds[i], bounds[i + 1])

    def join(i):
        join_halves(i, bounds[i], bounds[i + 1])

    def tokens_of(part, q):
        token_step(part, q, experts_left(q))

    def sums_of(q):
        sum_step(q, experts_left(q), True)

    own_rows()
    for copy in loads[1:]:
        copy.wait()
    full = hops - dense // 2
    token_step(0, 1, hops, False)

    @pl.loop(2, full + 1)
    def _(q):
        token_step(0, q, hops, True)

    send_own_block(1)
    for i in range(dense // 2):
        tokens_of(0, full + 1 + i)
        token_step(1, 1 + i, experts_left(1 + i), i > 0)
    some_experts(4)
    tokens_of(1, dense // 2 + 1)
    join(4)
    some_experts(0)

    @pl.loop(dense // 2 + 2, hops - dense + 1)
    def _(q):
        token_step(1, q, hops, True)

    join(0)
    tokens_of(1, hops - dense + 1)
    some_experts(1)
    back_hop = hops
    for q in range(hops - dense + 2, full + 1):
        sums_of(back_hop)
        back_hop -= 1
        tokens_of(1, q)
        if q == full - 1:
            join(1)
            some_experts(2)
    some_experts(3)
    join(2)
    join(3)
    while experts_left(back_hop) <= dense + 1:
        sums_of(back_hop)
        back_hop -= 1
    rest = back_hop

    @pl.loop(0, rest - 1)
    def _(i):
        sum_step(rest - i, hops, True)

    sum_step(1, hops, False)

    for d in (0, 1):
        for k in range(hops - d):
            m = hops - k - d
            rows, count = chunks(m)
            for c in range(min(m, dense)):
                token_copy(d, k, c).wait_send()
            for c in range(count):
                sum_copy(d, k + 1, c, rows).wait_send()
            meta_copy(d, k).wait_send()

    @pl.loop(0, n)
    def _(slot):
        row_copy(slot, t).wait_send()

    for i in range(5):
        part_copy(i, bounds[i] * per, (bounds[i + 1] - bounds[i]) * per).wait_send()

    total = dot(pw_own[...], res[slot_rows(0), :])
    for d in (1, 0):
        for c in range(tok_dev // big):
            sum_arrival(d, 0, c, big).wait_recv()
            total = total + dot(back[d][c], acc[d][0, span(c, big)])
    out_ref[...] = total.astype(BF16)


def per_device(tokens, picks, route_weights, gate_weight, up_weight, down_weight):
    n = lax.axis_size("ep")
    tok_dev, width = tokens.shape
    per = picks.shape[1]
    ff = down_weight.shape[1]
    dh = width // lax.axis_size("tp")
    hops = n // 2
    most = tok_dev // per
    dma = pltpu.SemaphoreType.DMA
    vmem = pltpu.VMEM
    kernel = pl.pallas_call(
        functools.partial(kernel_body, n, tok_dev, per, dh, ff),
        out_shape=jax.ShapeDtypeStruct((tok_dev, dh), BF16),
        in_specs=[
            pl.BlockSpec(memory_space=pl.ANY),
            pl.BlockSpec(memory_space=vmem),
            pl.BlockSpec(memory_space=vmem),
            pl.BlockSpec(memory_space=pl.ANY),
            pl.BlockSpec(memory_space=pl.ANY),
            pl.BlockSpec(memory_space=pl.ANY),
        ],
        out_specs=pl.BlockSpec(memory_space=vmem),
        scratch_shapes=[
            vmem((tok_dev, dh), BF16),
            vmem((width, ff), BF16),
            vmem((width, ff), BF16),
            vmem((ff, width), BF16),
            vmem((hops + 1, tok_dev, dh), BF16),
            vmem((hops, tok_dev, dh), BF16),
            vmem((hops + 1, per // 2, LANES), BF16),
            vmem((hops, per // 2, LANES), BF16),
            vmem((hops + 1, tok_dev, dh), BF16),
            vmem((hops, tok_dev, dh), BF16),
            vmem((2, n * per, dh), BF16),
            vmem((n * per, dh), BF16),
            vmem((n * per, dh), BF16),
            vmem((n * per, dh), BF16),
            vmem((hops + 1, tok_dev, per), BF16),
            vmem((hops, tok_dev, per), BF16),
            vmem((tok_dev, per), BF16),
            vmem((n * per, 1), F32),
            vmem((tok_dev // (2 * per), tok_dev, 2 * per), BF16),
            vmem((tok_dev // (2 * per), tok_dev, 2 * per), BF16),
            dma((4,)),
            dma((hops + 1, most)), dma((hops + 1, most)), dma((hops, most)), dma((hops, most)),
            dma((2, hops + 1)), dma((2, hops + 1)),
            dma((n,)), dma((n,)),
            dma((5,)), dma((5,)),
            dma((hops + 1, most)), dma((hops + 1, most)), dma((hops, most)), dma((hops, most)),
        ],
        compiler_params=pltpu.CompilerParams(
            collective_id=0, has_side_effects=True, vmem_limit_bytes=67043328
        ),
    )
    return kernel(tokens, picks, route_weights, gate_weight, up_weight, down_weight)


def solution(mesh):
    return jax.shard_map(
        per_device,
        mesh=mesh,
        in_specs=(
            P(("grp", "ep"), None),
            P(None, ("grp", "ep")),
            P(None, ("grp", "ep")),
            P("ep", None, "tp"),
            P("ep", None, "tp"),
            P("ep", "tp", None),
        ),
        out_specs=P(("grp", "ep"), "tp"),
        check_vma=False,
    )
```

```python
import functools

import jax
import jax.numpy as jnp
from jax import lax
from jax.experimental import pallas as pl
from jax.experimental.pallas import tpu as pltpu
from jax.sharding import PartitionSpec as P

F32 = jnp.float32
BF16 = jnp.bfloat16
LANES = 128
HALF_LANES = 64


def dot(a, b):
    return lax.dot_general(a, b, (((1,), (0,)), ((), ())), preferred_element_type=F32)


def dot_nt(a, b):
    return lax.dot_general(a, b, (((1,), (1,)), ((), ())), preferred_element_type=F32)


def iota(shape, dim):
    return lax.broadcasted_iota(jnp.int32, shape, dim)


def fiota(shape, dim):
    return iota(shape, dim).astype(F32)


def ones_where(cond):
    return jnp.where(cond, 1.0, 0.0)


def kernel_body(
    n, tok_dev, per, dh, ff,
    tok_hbm, picks_ref, rw_ref, wg_hbm, wu_hbm, wd_hbm, out_ref,
    tok, wg, wu, wd, buf_l, buf_s, met_l, met_s, acc_l, acc_s, x, res, pin, pout, pw_l, pw_s, pw_own, scale, hid,
    back_l, back_s, load_sem, sd_l, rd_l, sd_s, rd_s, sm, rm, sx, rx, sp, rp, sc_l, rc_l, sc_s, rc_s,
):
    hops = n // 2
    dense = tok_dev // per
    big = 2 * per
    z = lax.axis_index("ep")
    t = lax.axis_index("tp")
    sign = 1 - 2 * t
    ahead = (lax.rem(z + sign + n, n), lax.rem(z - sign + n, n))
    behind = (ahead[1], ahead[0])
    buf, met, acc = (buf_l, buf_s), (met_l, met_s), (acc_l, acc_s)
    pw, back = (pw_l, pw_s), (back_l, back_s)
    sd, rd, sc, rc = (sd_l, sd_s), (rd_l, rd_s), (sc_l, sc_s), (rc_l, rc_s)

    def remote(src, dst, s, r, where):
        return pltpu.make_async_remote_copy(
            src_ref=src, dst_ref=dst, send_sem=s, recv_sem=r,
            device_id=where, device_id_type=pl.DeviceIdType.MESH,
        )

    def chunks(m):
        return (big, tok_dev // big) if m > dense else (per, m)

    def rows_of(m):
        return min(tok_dev, per * m)

    def pieces(m, part):
        return range(part * (dense // 2), min(m, (part + 1) * (dense // 2)))

    def span(c, rows):
        return pl.ds(c * rows, rows)

    def token_copy(d, k, c):
        at = span(c, per)
        return remote(
            buf[d].at[k, at], buf[d].at[k + 1, at], sd[d].at[k, c], rd[d].at[k + 1, c], {"ep": ahead[d]}
        )

    def token_arrival(d, k, c):
        at = span(c, per)
        return remote(buf[d].at[k, at], buf[d].at[k, at], sd[d].at[k, c], rd[d].at[k, c], {"ep": ahead[d]})

    def meta_copy(d, k):
        return remote(met[d].at[k], met[d].at[k + 1], sm.at[d, k], rm.at[d, k + 1], {"ep": ahead[d]})

    def meta_arrival(d, k):
        return remote(met[d].at[k], met[d].at[k], sm.at[d, k], rm.at[d, k], {"ep": ahead[d]})

    def sum_copy(d, k, c, rows):
        at = span(c, rows)
        return remote(
            acc[d].at[k, at], acc[d].at[k - 1, at], sc[d].at[k, c], rc[d].at[k - 1, c], {"ep": behind[d]}
        )

    def sum_arrival(d, k, c, rows):
        at = span(c, rows)
        return remote(acc[d].at[k, at], acc[d].at[k, at], sc[d].at[k, c], rc[d].at[k, c], {"ep": behind[d]})

    def slot_rows(slot):
        return pl.ds(slot * per, per)

    def row_copy(slot, part):
        at = x.at[part, slot_rows(slot)]
        return remote(at, at, sx.at[slot], rx.at[slot], {"tp": 1 - t})

    def part_copy(i, r0, rows):
        at = pl.ds(r0, rows)
        return remote(pout.at[at], pin.at[at], sp.at[i], rp.at[i], {"tp": 1 - t})

    def slot_of(d, k):
        return 2 * k - 1 + t if d == 0 else 2 * k - t

    barrier = pltpu.get_barrier_semaphore()
    for where in ({"ep": ahead[0]}, {"ep": ahead[1]}, {"tp": 1 - t}):
        pl.semaphore_signal(barrier, inc=1, device_id=where, device_id_type=pl.DeviceIdType.MESH)
    my_half = pl.ds(pl.multiple_of(t * dh, dh), dh)
    its_half = pl.ds(pl.multiple_of((1 - t) * dh, dh), dh)
    loads = [
        pltpu.make_async_copy(tok_hbm.at[:, my_half], tok, load_sem.at[0]),
        pltpu.make_async_copy(wg_hbm.at[0], wg, load_sem.at[1]),
        pltpu.make_async_copy(wu_hbm.at[0], wu, load_sem.at[2]),
        pltpu.make_async_copy(wd_hbm.at[0], wd, load_sem.at[3]),
    ]
    for copy in loads:
        copy.start()

    ids = (picks_ref[...] - z * tok_dev).astype(F32).astype(BF16)
    eye = ones_where(iota((per, per), 0) == iota((per, per), 1)).astype(BF16)
    ids_t = dot_nt(eye, ids)
    spread = ones_where(iota((n, LANES), 1) == iota((n, LANES), 0) + n).astype(BF16)
    weights_t = dot(dot_nt(eye, rw_ref[...]).astype(BF16), spread)
    lane_e = iota((per, n), 1)
    lane_t = fiota((per, tok_dev), 1)
    meta_lane = iota((per, LANES), 1)

    def chosen_by(e):
        column = jnp.sum(jnp.where(lane_e == e, ids_t, 0.0), axis=1, keepdims=True)
        return column == lane_t

    def reach(e, far):
        member = jnp.max(ones_where(chosen_by(e)), axis=0, keepdims=True)
        d_long = lax.rem((e - z) * sign + n, n)
        d_short = lax.rem(n - d_long, n)
        d_long = jnp.where(d_long <= hops, d_long, 0).astype(F32)
        d_short = jnp.where(d_short < hops, d_short, 0).astype(F32)
        return jnp.maximum(far[0], member * d_long), jnp.maximum(far[1], member * d_short)

    zero_row = jnp.zeros((1, tok_dev), F32)
    trip = min(n, 8)

    def several(step):
        def run(i, carry):
            for j in range(trip):
                carry = step(i * trip + j, carry)
            return carry

        return run

    far = lax.fori_loop(0, n // trip, several(reach), (zero_row, zero_row))
    eye_t = ones_where(iota((tok_dev, tok_dev), 0) == iota((tok_dev, tok_dev), 1)).astype(BF16)
    sub_t = fiota((tok_dev, tok_dev), 0)
    keys, orders, swaps = [], [], []
    for d in (0, 1):
        wide = jnp.broadcast_to(far[d], (LANES, tok_dev)).astype(BF16)
        column = dot_nt(eye_t, wide)[:, :1]
        key_row = far[d] * tok_dev - fiota((1, tok_dev), 1)
        key_col = column * tok_dev - fiota((tok_dev, 1), 0)
        place_row = jnp.sum(ones_where(key_col > key_row), axis=0, keepdims=True)
        keys.append((key_row, key_col))
        orders.append(place_row)
        swaps.append(ones_where(place_row == sub_t).astype(BF16))

    def own_block(part):
        rows = tok_dev // 2
        for d in (0, 1):
            at = slice(part * rows, (part + 1) * rows)
            buf[d][0, at] = dot(swaps[d][at], tok[...]).astype(BF16)

    def send_own_block(part):
        for c in pieces(hops, part):
            for d in (0, 1):
                token_copy(d, 0, c).start()

    loads[0].wait()
    own_block(0)
    pl.semaphore_wait(barrier, 3)
    send_own_block(0)

    def place_ids(e, tiles):
        picked = chosen_by(e)
        out = []
        for d in (0, 1):
            column = jnp.sum(jnp.where(picked, orders[d], 0.0), axis=1, keepdims=True)
            out.append(tiles[d] + jnp.where(meta_lane == e, column, 0.0))
        return tuple(out)

    tiles = lax.fori_loop(0, n // trip, several(place_ids), (weights_t, weights_t))
    low = iota((per // 2, LANES), 1) < HALF_LANES
    for d in (0, 1):
        folded = jnp.where(low, tiles[d][: per // 2], pltpu.roll(tiles[d][per // 2 :], HALF_LANES, axis=1))
        met[d][0] = folded.astype(BF16)
    own_block(1)
    for d in (0, 1):
        meta_copy(d, 0).start()
        key_row, key_col = keys[d]
        place_col = jnp.sum(ones_where(key_row > key_col), axis=1, keepdims=True)
        for c in range(tok_dev // big):
            back[d][c] = ones_where(place_col == fiota((tok_dev, big), 1) + c * big).astype(BF16)

    def pick_rows(id_col, weight_col, block, slot, store_back, rows):
        scale[slot_rows(slot), :] = weight_col
        gather = ones_where(id_col == fiota((per, rows), 1)).astype(BF16)
        x[t, slot_rows(slot), :] = dot(gather, block).astype(BF16)
        row_copy(slot, t).start()
        square = iota((per, per), 0) == iota((per, per), 1)
        id_row = jnp.sum(jnp.where(square, id_col, 0.0), axis=0, keepdims=True)
        store_back(ones_where(fiota((rows, per), 0) == id_row).astype(BF16))

    def own_rows():
        id_col = jnp.sum(jnp.where(lane_e == z, ids_t, 0.0), axis=1, keepdims=True)
        weight_col = jnp.sum(jnp.where(meta_lane == z + n, weights_t, 0.0), axis=1, keepdims=True)

        def store(value):
            pw_own[...] = value

        pick_rows(id_col, weight_col, tok[...], 0, store, tok_dev)

    def arrived_rows(d, k, rows):
        tile = met[d][k].astype(F32)
        lane = iota((per // 2, LANES), 1)

        def column(at):
            parts = [
                jnp.sum(jnp.where(lane == at + part, tile, 0.0), axis=1, keepdims=True)
                for part in (0, HALF_LANES)
            ]
            return jnp.concatenate(parts, axis=0)

        def store(value):
            pw[d][k, :rows] = value

        slot = slot_of(d, k)
        if not isinstance(k, int):
            pass
        elif k == hops:
            slot = n - 1
        pick_rows(column(z), column(z + n), buf[d][k, :rows], slot, store, rows)

    def token_step(part, q, m, both=True, tasks=()):
        pairs = ((0, q), (1, q - 1)) if both else ((0, q),)
        onward = pieces(m - 1, part)
        arriving = pieces(m, part)
        for j, c in enumerate(arriving):
            for d, k in pairs:
                token_arrival(d, k, c).wait_recv()
                if c in onward:
                    token_copy(d, k, c).start()
            for task in tasks[j * len(tasks) // len(arriving) : (j + 1) * len(tasks) // len(arriving)]:
                task()
        if part == 0:
            for d, k in pairs:
                meta_arrival(d, k).wait_recv()
                if m > 1:
                    meta_copy(d, k).start()

    def take_rows(q):
        rows = rows_of(hops + 1 - q)
        pairs = ((0, q), (1, q - 1)) if q > 1 else ((0, q),)
        return [functools.partial(arrived_rows, d, k, rows) for d, k in pairs]

    fc = min(ff, 256)

    def feed_forward(i, first, last):
        r0, rows = first * per, (last - first) * per
        at = pl.ds(r0, rows)

        def enter():
            @pl.loop(first, last)
            def _(slot):
                row_copy(slot, 1 - t).wait_recv()

        def units(f):
            cols = pl.ds(f, fc)
            gate = dot(x[0, at, :], wg[:dh, cols]) + dot(x[1, at, :], wg[dh:, cols])
            up = dot(x[0, at, :], wu[:dh, cols]) + dot(x[1, at, :], wu[dh:, cols])
            hid[at, cols] = (gate / (1.0 + jnp.exp(-gate)) * up * scale[at, :]).astype(BF16)

        def down_for_partner():
            pout[at, :] = dot(hid[at, :], wd[:, its_half]).astype(BF16)
            part_copy(i, r0, rows).start()

        def down():
            res[at, :] = dot(hid[at, :], wd[:, my_half]).astype(BF16)

        blocks = [functools.partial(units, f) for f in range(0, ff, fc)]
        return [enter] + blocks + [down_for_partner, down]

    def join_halves(i, first, last):
        r0, rows = first * per, (last - first) * per
        at = pl.ds(r0, rows)
        part_copy(i, r0, rows).wait_recv()
        res[at, :] = (res[at, :].astype(F32) + pin[at, :].astype(F32)).astype(BF16)

    def add_to(d, k, slot, at):
        return dot(pw[d][k, at], res[slot_rows(slot), :])

    def sum_step(q, m, both):
        pairs = ((0, q), (1, q - 1)) if both else ((0, q),)
        rows_out, n_out = chunks(m)
        rows_in, n_in = chunks(m - 1)
        each = rows_out // rows_in
        order = [n_out - 1] + list(range(n_out - 1)) if m <= dense else list(range(n_out))
        for c in order:
            for d, k in pairs:
                slot = slot_of(d, k)
                if isinstance(k, int) and k == hops:
                    slot = n - 1
                at = span(c, rows_out)
                value = add_to(d, k, slot, at)
                if c * each < n_in:
                    for piece in range(c * each, (c + 1) * each):
                        sum_arrival(d, k, piece, rows_in).wait_recv()
                    value = value + acc[d][k, at].astype(F32)
                acc[d][k, at] = value.astype(BF16)
                sum_copy(d, k, c, rows_out).start()

    def experts_left(q):
        return hops + 1 - q

    bounds = [0] + [2 * k - 1 for k in (hops // 4, 7 * hops // 16, 5 * hops // 8, 13 * hops // 16)] + [n]

    def some_experts(i):
        return feed_forward(i, bounds[i], bounds[i + 1])

    def join(i):
        join_halves(i, bounds[i], bounds[i + 1])

    def tokens_of(part, q, tasks=()):
        token_step(part, q, experts_left(q), q > 1, tasks)

    def run(tasks):
        for task in tasks:
            task()

    def joined(i):
        return functools.partial(join, i)

    def sums_of(q):
        sum_step(q, experts_left(q), True)

    own_rows()
    for copy in loads[1:]:
        copy.wait()
    full = hops - dense // 2
    token_step(0, 1, hops, False)

    @pl.loop(2, full + 1)
    def _(q):
        token_step(0, q, hops, True)

    send_own_block(1)
    near = 0
    for q in range(full + 1, hops + 1):
        tokens_of(0, q)
        tokens_of(1, near + 1, take_rows(q) + (take_rows(near) if near else []))
        near += 1
    far_tasks, near_tasks = some_experts(4), some_experts(0)
    tokens_of(1, near + 1, take_rows(near) + far_tasks[:2])
    tokens_of(1, near + 2, take_rows(near + 1) + far_tasks[2:])
    tokens_of(1, near + 3, take_rows(near + 2) + [joined(4)] + near_tasks[:2])
    tokens_of(1, near + 4, take_rows(near + 3) + near_tasks[2:])
    tokens_of(1, near + 5, take_rows(near + 4) + some_experts(1) + [joined(0)])
    run(take_rows(near + 5))
    back_hop = hops
    for q in range(near + 6, full + 1):
        sums_of(back_hop)
        back_hop -= 1
        tokens_of(1, q)
        run(take_rows(q))
        if q == full - 2:
            join(1)
            run(some_experts(2))
    run(some_experts(3))
    join(2)
    join(3)
    while experts_left(back_hop) <= dense + 1:
        sums_of(back_hop)
        back_hop -= 1
    rest = back_hop

    @pl.loop(0, rest - 1)
    def _(i):
        sum_step(rest - i, hops, True)

    sum_step(1, hops, False)

    for d in (0, 1):
        for k in range(hops - d):
            m = hops - k - d
            rows, count = chunks(m)
            for c in range(min(m, dense)):
                token_copy(d, k, c).wait_send()
            for c in range(count):
                sum_copy(d, k + 1, c, rows).wait_send()
            meta_copy(d, k).wait_send()

    @pl.loop(0, n)
    def _(slot):
        row_copy(slot, t).wait_send()

    for i in range(5):
        part_copy(i, bounds[i] * per, (bounds[i + 1] - bounds[i]) * per).wait_send()

    total = dot(pw_own[...], res[slot_rows(0), :])
    for d in (1, 0):
        for c in range(tok_dev // big):
            sum_arrival(d, 0, c, big).wait_recv()
            total = total + dot(back[d][c], acc[d][0, span(c, big)])
    out_ref[...] = total.astype(BF16)


def per_device(tokens, picks, route_weights, gate_weight, up_weight, down_weight):
    n = lax.axis_size("ep")
    tok_dev, width = tokens.shape
    per = picks.shape[1]
    ff = down_weight.shape[1]
    dh = width // lax.axis_size("tp")
    hops = n // 2
    most = tok_dev // per
    dma = pltpu.SemaphoreType.DMA
    vmem = pltpu.VMEM
    kernel = pl.pallas_call(
        functools.partial(kernel_body, n, tok_dev, per, dh, ff),
        out_shape=jax.ShapeDtypeStruct((tok_dev, dh), BF16),
        in_specs=[
            pl.BlockSpec(memory_space=pl.ANY),
            pl.BlockSpec(memory_space=vmem),
            pl.BlockSpec(memory_space=vmem),
            pl.BlockSpec(memory_space=pl.ANY),
            pl.BlockSpec(memory_space=pl.ANY),
            pl.BlockSpec(memory_space=pl.ANY),
        ],
        out_specs=pl.BlockSpec(memory_space=vmem),
        scratch_shapes=[
            vmem((tok_dev, dh), BF16),
            vmem((width, ff), BF16),
            vmem((width, ff), BF16),
            vmem((ff, width), BF16),
            vmem((hops + 1, tok_dev, dh), BF16),
            vmem((hops, tok_dev, dh), BF16),
            vmem((hops + 1, per // 2, LANES), BF16),
            vmem((hops, per // 2, LANES), BF16),
            vmem((hops + 1, tok_dev, dh), BF16),
            vmem((hops, tok_dev, dh), BF16),
            vmem((2, n * per, dh), BF16),
            vmem((n * per, dh), BF16),
            vmem((n * per, dh), BF16),
            vmem((n * per, dh), BF16),
            vmem((hops + 1, tok_dev, per), BF16),
            vmem((hops, tok_dev, per), BF16),
            vmem((tok_dev, per), BF16),
            vmem((n * per, 1), F32),
            vmem((n * per, ff), BF16),
            vmem((tok_dev // (2 * per), tok_dev, 2 * per), BF16),
            vmem((tok_dev // (2 * per), tok_dev, 2 * per), BF16),
            dma((4,)),
            dma((hops + 1, most)), dma((hops + 1, most)), dma((hops, most)), dma((hops, most)),
            dma((2, hops + 1)), dma((2, hops + 1)),
            dma((n,)), dma((n,)),
            dma((5,)), dma((5,)),
            dma((hops + 1, most)), dma((hops + 1, most)), dma((hops, most)), dma((hops, most)),
        ],
        compiler_params=pltpu.CompilerParams(
            collective_id=0, has_side_effects=True, vmem_limit_bytes=67043328
        ),
    )
    return kernel(tokens, picks, route_weights, gate_weight, up_weight, down_weight)


def solution(mesh):
    return jax.shard_map(
        per_device,
        mesh=mesh,
        in_specs=(
            P(("grp", "ep"), None),
            P(None, ("grp", "ep")),
            P(None, ("grp", "ep")),
            P("ep", None, "tp"),
            P("ep", None, "tp"),
            P("ep", "tp", None),
        ),
        out_specs=P(("grp", "ep"), "tp"),
        check_vma=False,
    )
```

```python
import functools

import jax
import jax.numpy as jnp
from jax import lax
from jax.experimental import pallas as pl
from jax.experimental.pallas import tpu as pltpu
from jax.sharding import PartitionSpec as P

F32 = jnp.float32
BF16 = jnp.bfloat16
LANES = 128
HALF_LANES = 64


def dot(a, b):
    return lax.dot_general(a, b, (((1,), (0,)), ((), ())), preferred_element_type=F32)


def dot_nt(a, b):
    return lax.dot_general(a, b, (((1,), (1,)), ((), ())), preferred_element_type=F32)


def iota(shape, dim):
    return lax.broadcasted_iota(jnp.int32, shape, dim)


def fiota(shape, dim):
    return iota(shape, dim).astype(F32)


def ones_where(cond):
    return jnp.where(cond, 1.0, 0.0)


def kernel_body(
    n, tok_dev, per, dh, ff,
    tok_hbm, picks_ref, rw_ref, wg_hbm, wu_hbm, wd_hbm, out_ref,
    tok, wg, wu, wd, buf_l, buf_s, met_l, met_s, acc_l, acc_s, x, res, pin, pout, pw_l, pw_s, pw_own, scale,
    back_l, back_s, load_sem, sd_l, rd_l, sd_s, rd_s, sm, rm, sx, rx, sp, rp, sc_l, rc_l, sc_s, rc_s,
):
    hops = n // 2
    dense = tok_dev // per
    big = 2 * per
    z = lax.axis_index("ep")
    t = lax.axis_index("tp")
    sign = 1 - 2 * t
    ahead = (lax.rem(z + sign + n, n), lax.rem(z - sign + n, n))
    behind = (ahead[1], ahead[0])
    buf, met, acc = (buf_l, buf_s), (met_l, met_s), (acc_l, acc_s)
    pw, back = (pw_l, pw_s), (back_l, back_s)
    sd, rd, sc, rc = (sd_l, sd_s), (rd_l, rd_s), (sc_l, sc_s), (rc_l, rc_s)

    def remote(src, dst, s, r, where):
        return pltpu.make_async_remote_copy(
            src_ref=src, dst_ref=dst, send_sem=s, recv_sem=r,
            device_id=where, device_id_type=pl.DeviceIdType.MESH,
        )

    def chunks(m):
        return (big, tok_dev // big) if m > dense else (per, m)

    def rows_of(m):
        return min(tok_dev, per * m)

    def pieces(m, part):
        return range(part * (dense // 2), min(m, (part + 1) * (dense // 2)))

    def span(c, rows):
        return pl.ds(c * rows, rows)

    def token_copy(d, k, c):
        at = span(c, per)
        return remote(
            buf[d].at[k, at], buf[d].at[k + 1, at], sd[d].at[k, c], rd[d].at[k + 1, c], {"ep": ahead[d]}
        )

    def token_arrival(d, k, c):
        at = span(c, per)
        return remote(buf[d].at[k, at], buf[d].at[k, at], sd[d].at[k, c], rd[d].at[k, c], {"ep": ahead[d]})

    def meta_copy(d, k):
        return remote(met[d].at[k], met[d].at[k + 1], sm.at[d, k], rm.at[d, k + 1], {"ep": ahead[d]})

    def meta_arrival(d, k):
        return remote(met[d].at[k], met[d].at[k], sm.at[d, k], rm.at[d, k], {"ep": ahead[d]})

    def sum_copy(d, k, c, rows):
        at = span(c, rows)
        return remote(
            acc[d].at[k, at], acc[d].at[k - 1, at], sc[d].at[k, c], rc[d].at[k - 1, c], {"ep": behind[d]}
        )

    def sum_arrival(d, k, c, rows):
        at = span(c, rows)
        return remote(acc[d].at[k, at], acc[d].at[k, at], sc[d].at[k, c], rc[d].at[k, c], {"ep": behind[d]})

    def slot_rows(slot):
        return pl.ds(slot * per, per)

    def row_copy(slot, part):
        at = x.at[part, slot_rows(slot)]
        return remote(at, at, sx.at[slot], rx.at[slot], {"tp": 1 - t})

    def part_copy(i, r0, rows):
        at = pl.ds(r0, rows)
        return remote(pout.at[at], pin.at[at], sp.at[i], rp.at[i], {"tp": 1 - t})

    def slot_of(d, k):
        return 2 * k - 1 + t if d == 0 else 2 * k - t

    barrier = pltpu.get_barrier_semaphore()
    for where in ({"ep": ahead[0]}, {"ep": ahead[1]}, {"tp": 1 - t}):
        pl.semaphore_signal(barrier, inc=1, device_id=where, device_id_type=pl.DeviceIdType.MESH)
    my_half = pl.ds(pl.multiple_of(t * dh, dh), dh)
    its_half = pl.ds(pl.multiple_of((1 - t) * dh, dh), dh)
    loads = [
        pltpu.make_async_copy(tok_hbm.at[:, my_half], tok, load_sem.at[0]),
        pltpu.make_async_copy(wg_hbm.at[0], wg, load_sem.at[1]),
        pltpu.make_async_copy(wu_hbm.at[0], wu, load_sem.at[2]),
        pltpu.make_async_copy(wd_hbm.at[0], wd, load_sem.at[3]),
    ]
    for copy in loads:
        copy.start()

    ids = (picks_ref[...] - z * tok_dev).astype(F32).astype(BF16)
    eye = ones_where(iota((per, per), 0) == iota((per, per), 1)).astype(BF16)
    ids_t = dot_nt(eye, ids)
    spread = ones_where(iota((n, LANES), 1) == iota((n, LANES), 0) + n).astype(BF16)
    weights_t = dot(dot_nt(eye, rw_ref[...]).astype(BF16), spread)
    lane_e = iota((per, n), 1)
    lane_t = fiota((per, tok_dev), 1)
    meta_lane = iota((per, LANES), 1)

    def chosen_by(e):
        column = jnp.sum(jnp.where(lane_e == e, ids_t, 0.0), axis=1, keepdims=True)
        return column == lane_t

    def reach(e, far):
        member = jnp.max(ones_where(chosen_by(e)), axis=0, keepdims=True)
        d_long = lax.rem((e - z) * sign + n, n)
        d_short = lax.rem(n - d_long, n)
        d_long = jnp.where(d_long <= hops, d_long, 0).astype(F32)
        d_short = jnp.where(d_short < hops, d_short, 0).astype(F32)
        return jnp.maximum(far[0], member * d_long), jnp.maximum(far[1], member * d_short)

    zero_row = jnp.zeros((1, tok_dev), F32)
    trip = min(n, 8)

    def several(step):
        def run(i, carry):
            for j in range(trip):
                carry = step(i * trip + j, carry)
            return carry

        return run

    far = lax.fori_loop(0, n // trip, several(reach), (zero_row, zero_row))
    eye_t = ones_where(iota((tok_dev, tok_dev), 0) == iota((tok_dev, tok_dev), 1)).astype(BF16)
    sub_t = fiota((tok_dev, tok_dev), 0)
    keys, orders, swaps = [], [], []
    for d in (0, 1):
        wide = jnp.broadcast_to(far[d], (LANES, tok_dev)).astype(BF16)
        column = dot_nt(eye_t, wide)[:, :1]
        key_row = far[d] * tok_dev - fiota((1, tok_dev), 1)
        key_col = column * tok_dev - fiota((tok_dev, 1), 0)
        place_row = jnp.sum(ones_where(key_col > key_row), axis=0, keepdims=True)
        keys.append((key_row, key_col))
        orders.append(place_row)
        swaps.append(ones_where(place_row == sub_t).astype(BF16))

    def own_block(part):
        rows = tok_dev // 2
        for d in (0, 1):
            at = slice(part * rows, (part + 1) * rows)
            buf[d][0, at] = dot(swaps[d][at], tok[...]).astype(BF16)

    def send_own_block(part):
        for c in pieces(hops, part):
            for d in (0, 1):
                token_copy(d, 0, c).start()

    loads[0].wait()
    own_block(0)
    pl.semaphore_wait(barrier, 3)
    send_own_block(0)

    def place_ids(e, tiles):
        picked = chosen_by(e)
        out = []
        for d in (0, 1):
            column = jnp.sum(jnp.where(picked, orders[d], 0.0), axis=1, keepdims=True)
            out.append(tiles[d] + jnp.where(meta_lane == e, column, 0.0))
        return tuple(out)

    tiles = lax.fori_loop(0, n // trip, several(place_ids), (weights_t, weights_t))
    low = iota((per // 2, LANES), 1) < HALF_LANES
    for d in (0, 1):
        folded = jnp.where(low, tiles[d][: per // 2], pltpu.roll(tiles[d][per // 2 :], HALF_LANES, axis=1))
        met[d][0] = folded.astype(BF16)
    own_block(1)
    for d in (0, 1):
        meta_copy(d, 0).start()
        key_row, key_col = keys[d]
        place_col = jnp.sum(ones_where(key_row > key_col), axis=1, keepdims=True)
        for c in range(tok_dev // big):
            back[d][c] = ones_where(place_col == fiota((tok_dev, big), 1) + c * big).astype(BF16)

    def pick_rows(id_col, weight_col, block, slot, store_back, rows):
        scale[slot_rows(slot), :] = weight_col
        gather = ones_where(id_col == fiota((per, rows), 1)).astype(BF16)
        x[t, slot_rows(slot), :] = dot(gather, block).astype(BF16)
        row_copy(slot, t).start()
        square = iota((per, per), 0) == iota((per, per), 1)
        id_row = jnp.sum(jnp.where(square, id_col, 0.0), axis=0, keepdims=True)
        store_back(ones_where(fiota((rows, per), 0) == id_row).astype(BF16))

    def own_rows():
        id_col = jnp.sum(jnp.where(lane_e == z, ids_t, 0.0), axis=1, keepdims=True)
        weight_col = jnp.sum(jnp.where(meta_lane == z + n, weights_t, 0.0), axis=1, keepdims=True)

        def store(value):
            pw_own[...] = value

        pick_rows(id_col, weight_col, tok[...], 0, store, tok_dev)

    def arrived_rows(d, k, rows):
        tile = met[d][k].astype(F32)
        lane = iota((per // 2, LANES), 1)

        def column(at):
            parts = [
                jnp.sum(jnp.where(lane == at + part, tile, 0.0), axis=1, keepdims=True)
                for part in (0, HALF_LANES)
            ]
            return jnp.concatenate(parts, axis=0)

        def store(value):
            pw[d][k, :rows] = value

        slot = slot_of(d, k)
        if not isinstance(k, int):
            pass
        elif k == hops:
            slot = n - 1
        pick_rows(column(z), column(z + n), buf[d][k, :rows], slot, store, rows)

    def token_step(part, q, m, both=True):
        pairs = ((0, q), (1, q - 1)) if both else ((0, q),)
        onward = pieces(m - 1, part)
        for c in pieces(m, part):
            for d, k in pairs:
                token_arrival(d, k, c).wait_recv()
                if c in onward:
                    token_copy(d, k, c).start()
        if part == 0:
            for d, k in pairs:
                meta_arrival(d, k).wait_recv()
                if m > 1:
                    meta_copy(d, k).start()
        if part == (0 if m <= dense // 2 else 1):
            for d, k in pairs:
                arrived_rows(d, k, rows_of(m))

    fc = min(ff, 256)

    def feed_forward(i, first, last):
        r0, rows = first * per, (last - first) * per

        @pl.loop(first, last)
        def _(slot):
            row_copy(slot, 1 - t).wait_recv()

        at = pl.ds(r0, rows)
        hidden = []
        for f in range(0, ff, fc):
            cols = pl.ds(f, fc)
            gate = dot(x[0, at, :], wg[:dh, cols]) + dot(x[1, at, :], wg[dh:, cols])
            up = dot(x[0, at, :], wu[:dh, cols]) + dot(x[1, at, :], wu[dh:, cols])
            hidden.append((gate / (1.0 + jnp.exp(-gate)) * up * scale[at, :]).astype(BF16))
        hidden = jnp.concatenate(hidden, axis=1)
        pout[at, :] = dot(hidden, wd[:, its_half]).astype(BF16)
        part_copy(i, r0, rows).start()
        res[at, :] = dot(hidden, wd[:, my_half]).astype(BF16)

    def join_halves(i, first, last):
        r0, rows = first * per, (last - first) * per
        at = pl.ds(r0, rows)
        part_copy(i, r0, rows).wait_recv()
        res[at, :] = (res[at, :].astype(F32) + pin[at, :].astype(F32)).astype(BF16)

    def add_to(d, k, slot, at):
        return dot(pw[d][k, at], res[slot_rows(slot), :])

    def sum_step(q, m, both):
        pairs = ((0, q), (1, q - 1)) if both else ((0, q),)
        rows_out, n_out = chunks(m)
        rows_in, n_in = chunks(m - 1)
        each = rows_out // rows_in
        order = [n_out - 1] + list(range(n_out - 1)) if m <= dense else list(range(n_out))
        for c in order:
            for d, k in pairs:
                slot = slot_of(d, k)
                if isinstance(k, int) and k == hops:
                    slot = n - 1
                at = span(c, rows_out)
                value = add_to(d, k, slot, at)
                if c * each < n_in:
                    for piece in range(c * each, (c + 1) * each):
                        sum_arrival(d, k, piece, rows_in).wait_recv()
                    value = value + acc[d][k, at].astype(F32)
                acc[d][k, at] = value.astype(BF16)
                sum_copy(d, k, c, rows_out).start()

    def experts_left(q):
        return hops + 1 - q

    bounds = [0, hops // 2 - 1, hops - 1, 5 * hops // 4 + 1, 3 * hops // 2 + 1, n]

    def some_experts(i):
        feed_forward(i, bounds[i], bounds[i + 1])

    def join(i):
        join_halves(i, bounds[i], bounds[i + 1])

    def tokens_of(part, q):
        token_step(part, q, experts_left(q), q > 1)

    def sums_of(q):
        sum_step(q, experts_left(q), True)

    own_rows()
    for copy in loads[1:]:
        copy.wait()
    full = hops - dense // 2
    alone = full - 2
    token_step(0, 1, hops, False)

    @pl.loop(2, alone + 1)
    def _(q):
        token_step(0, q, hops, True)

    send_own_block(1)
    near = 1
    for q in range(alone + 1, hops + 1):
        tokens_of(0, q)
        tokens_of(1, near)
        if near == hops // 4 + 1:
            some_experts(0)
        near += 1
    some_experts(4)
    tokens_of(1, near)
    join(0)
    join(4)
    for q in range(near + 1, hops - dense + 1):
        tokens_of(1, q)
    tokens_of(1, hops - dense + 1)
    back_hop = hops
    for q in range(hops - dense + 2, full + 1):
        sums_of(back_hop)
        back_hop -= 1
        if q == hops - dense + 2:
            some_experts(1)
        tokens_of(1, q)
        if q == full - 1:
            join(1)
            some_experts(2)
    some_experts(3)
    join(2)
    join(3)
    while experts_left(back_hop) <= dense + 1:
        sums_of(back_hop)
        back_hop -= 1
    rest = back_hop

    @pl.loop(0, rest - 1)
    def _(i):
        sum_step(rest - i, hops, True)

    sum_step(1, hops, False)

    for d in (0, 1):
        for k in range(hops - d):
            m = hops - k - d
            rows, count = chunks(m)
            for c in range(min(m, dense)):
                token_copy(d, k, c).wait_send()
            for c in range(count):
                sum_copy(d, k + 1, c, rows).wait_send()
            meta_copy(d, k).wait_send()

    @pl.loop(0, n)
    def _(slot):
        row_copy(slot, t).wait_send()

    for i in range(5):
        part_copy(i, bounds[i] * per, (bounds[i + 1] - bounds[i]) * per).wait_send()

    total = dot(pw_own[...], res[slot_rows(0), :])
    for d in (1, 0):
        for c in range(tok_dev // big):
            sum_arrival(d, 0, c, big).wait_recv()
            total = total + dot(back[d][c], acc[d][0, span(c, big)])
    out_ref[...] = total.astype(BF16)


def per_device(tokens, picks, route_weights, gate_weight, up_weight, down_weight):
    n = lax.axis_size("ep")
    tok_dev, width = tokens.shape
    per = picks.shape[1]
    ff = down_weight.shape[1]
    dh = width // lax.axis_size("tp")
    hops = n // 2
    most = tok_dev // per
    dma = pltpu.SemaphoreType.DMA
    vmem = pltpu.VMEM
    kernel = pl.pallas_call(
        functools.partial(kernel_body, n, tok_dev, per, dh, ff),
        out_shape=jax.ShapeDtypeStruct((tok_dev, dh), BF16),
        in_specs=[
            pl.BlockSpec(memory_space=pl.ANY),
            pl.BlockSpec(memory_space=vmem),
            pl.BlockSpec(memory_space=vmem),
            pl.BlockSpec(memory_space=pl.ANY),
            pl.BlockSpec(memory_space=pl.ANY),
            pl.BlockSpec(memory_space=pl.ANY),
        ],
        out_specs=pl.BlockSpec(memory_space=vmem),
        scratch_shapes=[
            vmem((tok_dev, dh), BF16),
            vmem((width, ff), BF16),
            vmem((width, ff), BF16),
            vmem((ff, width), BF16),
            vmem((hops + 1, tok_dev, dh), BF16),
            vmem((hops, tok_dev, dh), BF16),
            vmem((hops + 1, per // 2, LANES), BF16),
            vmem((hops, per // 2, LANES), BF16),
            vmem((hops + 1, tok_dev, dh), BF16),
            vmem((hops, tok_dev, dh), BF16),
            vmem((2, n * per, dh), BF16),
            vmem((n * per, dh), BF16),
            vmem((n * per, dh), BF16),
            vmem((n * per, dh), BF16),
            vmem((hops + 1, tok_dev, per), BF16),
            vmem((hops, tok_dev, per), BF16),
            vmem((tok_dev, per), BF16),
            vmem((n * per, 1), F32),
            vmem((tok_dev // (2 * per), tok_dev, 2 * per), BF16),
            vmem((tok_dev // (2 * per), tok_dev, 2 * per), BF16),
            dma((4,)),
            dma((hops + 1, most)), dma((hops + 1, most)), dma((hops, most)), dma((hops, most)),
            dma((2, hops + 1)), dma((2, hops + 1)),
            dma((n,)), dma((n,)),
            dma((5,)), dma((5,)),
            dma((hops + 1, most)), dma((hops + 1, most)), dma((hops, most)), dma((hops, most)),
        ],
        compiler_params=pltpu.CompilerParams(
            collective_id=0, has_side_effects=True, vmem_limit_bytes=67043328
        ),
    )
    return kernel(tokens, picks, route_weights, gate_weight, up_weight, down_weight)


def solution(mesh):
    return jax.shard_map(
        per_device,
        mesh=mesh,
        in_specs=(
            P(("grp", "ep"), None),
            P(None, ("grp", "ep")),
            P(None, ("grp", "ep")),
            P("ep", None, "tp"),
            P("ep", None, "tp"),
            P("ep", "tp", None),
        ),
        out_specs=P(("grp", "ep"), "tp"),
        check_vma=False,
    )
```

```python
import functools

import jax
import jax.numpy as jnp
from jax import lax
from jax.experimental import pallas as pl
from jax.experimental.pallas import tpu as pltpu
from jax.sharding import PartitionSpec as P

F32 = jnp.float32
BF16 = jnp.bfloat16
LANES = 128
HALF_LANES = 64


def dot(a, b):
    return lax.dot_general(a, b, (((1,), (0,)), ((), ())), preferred_element_type=F32)


def dot_nt(a, b):
    return lax.dot_general(a, b, (((1,), (1,)), ((), ())), preferred_element_type=F32)


def iota(shape, dim):
    return lax.broadcasted_iota(jnp.int32, shape, dim)


def fiota(shape, dim):
    return iota(shape, dim).astype(F32)


def ones_where(cond):
    return jnp.where(cond, 1.0, 0.0)


def kernel_body(
    n, tok_dev, per, dh, ff,
    tok_hbm, picks_ref, rw_ref, wg_hbm, wu_hbm, wd_hbm, out_ref,
    tok, wg, wu, wd, buf_l, buf_s, met_l, met_s, acc_l, acc_s, x, res, pin, pout, pw_l, pw_s, pw_own, scale,
    back_l, back_s, load_sem, sd_l, rd_l, sd_s, rd_s, sm, rm, sx, rx, sp, rp, sc_l, rc_l, sc_s, rc_s,
):
    hops = n // 2
    dense = tok_dev // per
    big = 2 * per
    z = lax.axis_index("ep")
    t = lax.axis_index("tp")
    sign = 1 - 2 * t
    ahead = (lax.rem(z + sign + n, n), lax.rem(z - sign + n, n))
    behind = (ahead[1], ahead[0])
    buf, met, acc = (buf_l, buf_s), (met_l, met_s), (acc_l, acc_s)
    pw, back = (pw_l, pw_s), (back_l, back_s)
    sd, rd, sc, rc = (sd_l, sd_s), (rd_l, rd_s), (sc_l, sc_s), (rc_l, rc_s)

    def remote(src, dst, s, r, where):
        return pltpu.make_async_remote_copy(
            src_ref=src, dst_ref=dst, send_sem=s, recv_sem=r,
            device_id=where, device_id_type=pl.DeviceIdType.MESH,
        )

    def chunks(m):
        return (big, tok_dev // big) if m > dense else (per, m)

    def rows_of(m):
        return min(tok_dev, per * m)

    def pieces(m, part):
        return range(part * (dense // 2), min(m, (part + 1) * (dense // 2)))

    def span(c, rows):
        return pl.ds(c * rows, rows)

    def token_copy(d, k, c):
        at = span(c, per)
        return remote(
            buf[d].at[k, at], buf[d].at[k + 1, at], sd[d].at[k, c], rd[d].at[k + 1, c], {"ep": ahead[d]}
        )

    def token_arrival(d, k, c):
        at = span(c, per)
        return remote(buf[d].at[k, at], buf[d].at[k, at], sd[d].at[k, c], rd[d].at[k, c], {"ep": ahead[d]})

    def meta_copy(d, k):
        return remote(met[d].at[k], met[d].at[k + 1], sm.at[d, k], rm.at[d, k + 1], {"ep": ahead[d]})

    def meta_arrival(d, k):
        return remote(met[d].at[k], met[d].at[k], sm.at[d, k], rm.at[d, k], {"ep": ahead[d]})

    def sum_copy(d, k, c, rows):
        at = span(c, rows)
        return remote(
            acc[d].at[k, at], acc[d].at[k - 1, at], sc[d].at[k, c], rc[d].at[k - 1, c], {"ep": behind[d]}
        )

    def sum_arrival(d, k, c, rows):
        at = span(c, rows)
        return remote(acc[d].at[k, at], acc[d].at[k, at], sc[d].at[k, c], rc[d].at[k, c], {"ep": behind[d]})

    def slot_rows(slot):
        return pl.ds(slot * per, per)

    def row_copy(slot, part):
        at = x.at[part, slot_rows(slot)]
        return remote(at, at, sx.at[slot], rx.at[slot], {"tp": 1 - t})

    def part_copy(i, r0, rows):
        at = pl.ds(r0, rows)
        return remote(pout.at[at], pin.at[at], sp.at[i], rp.at[i], {"tp": 1 - t})

    def slot_of(d, k):
        return 2 * k - 1 + t if d == 0 else 2 * k - t

    barrier = pltpu.get_barrier_semaphore()
    for where in ({"ep": ahead[0]}, {"ep": ahead[1]}, {"tp": 1 - t}):
        pl.semaphore_signal(barrier, inc=1, device_id=where, device_id_type=pl.DeviceIdType.MESH)
    my_half = pl.ds(pl.multiple_of(t * dh, dh), dh)
    its_half = pl.ds(pl.multiple_of((1 - t) * dh, dh), dh)
    loads = [
        pltpu.make_async_copy(tok_hbm.at[:, my_half], tok, load_sem.at[0]),
        pltpu.make_async_copy(wg_hbm.at[0], wg, load_sem.at[1]),
        pltpu.make_async_copy(wu_hbm.at[0], wu, load_sem.at[2]),
        pltpu.make_async_copy(wd_hbm.at[0], wd, load_sem.at[3]),
    ]
    for copy in loads:
        copy.start()

    ids = (picks_ref[...] - z * tok_dev).astype(F32).astype(BF16)
    eye = ones_where(iota((per, per), 0) == iota((per, per), 1)).astype(BF16)
    ids_t = dot_nt(eye, ids)
    spread = ones_where(iota((n, LANES), 1) == iota((n, LANES), 0) + n).astype(BF16)
    weights_t = dot(dot_nt(eye, rw_ref[...]).astype(BF16), spread)
    lane_e = iota((per, n), 1)
    lane_t = fiota((per, tok_dev), 1)
    meta_lane = iota((per, LANES), 1)

    def chosen_by(e):
        column = jnp.sum(jnp.where(lane_e == e, ids_t, 0.0), axis=1, keepdims=True)
        return column == lane_t

    def reach(e, far):
        member = jnp.max(ones_where(chosen_by(e)), axis=0, keepdims=True)
        d_long = lax.rem((e - z) * sign + n, n)
        d_short = lax.rem(n - d_long, n)
        d_long = jnp.where(d_long <= hops, d_long, 0).astype(F32)
        d_short = jnp.where(d_short < hops, d_short, 0).astype(F32)
        return jnp.maximum(far[0], member * d_long), jnp.maximum(far[1], member * d_short)

    zero_row = jnp.zeros((1, tok_dev), F32)
    trip = min(n, 8)

    def several(step):
        def run(i, carry):
            for j in range(trip):
                carry = step(i * trip + j, carry)
            return carry

        return run

    far = lax.fori_loop(0, n // trip, several(reach), (zero_row, zero_row))
    eye_t = ones_where(iota((tok_dev, tok_dev), 0) == iota((tok_dev, tok_dev), 1)).astype(BF16)
    sub_t = fiota((tok_dev, tok_dev), 0)
    keys, orders, swaps = [], [], []
    for d in (0, 1):
        wide = jnp.broadcast_to(far[d], (LANES, tok_dev)).astype(BF16)
        column = dot_nt(eye_t, wide)[:, :1]
        key_row = far[d] * tok_dev - fiota((1, tok_dev), 1)
        key_col = column * tok_dev - fiota((tok_dev, 1), 0)
        place_row = jnp.sum(ones_where(key_col > key_row), axis=0, keepdims=True)
        keys.append((key_row, key_col))
        orders.append(place_row)
        swaps.append(ones_where(place_row == sub_t).astype(BF16))

    def own_block(part):
        rows = tok_dev // 2
        for d in (0, 1):
            at = slice(part * rows, (part + 1) * rows)
            buf[d][0, at] = dot(swaps[d][at], tok[...]).astype(BF16)

    def send_own_block(part):
        for c in pieces(hops, part):
            for d in (0, 1):
                token_copy(d, 0, c).start()

    loads[0].wait()
    own_block(0)
    pl.semaphore_wait(barrier, 3)
    send_own_block(0)

    def place_ids(e, tiles):
        picked = chosen_by(e)
        out = []
        for d in (0, 1):
            column = jnp.sum(jnp.where(picked, orders[d], 0.0), axis=1, keepdims=True)
            out.append(tiles[d] + jnp.where(meta_lane == e, column, 0.0))
        return tuple(out)

    tiles = lax.fori_loop(0, n // trip, several(place_ids), (weights_t, weights_t))
    low = iota((per // 2, LANES), 1) < HALF_LANES
    for d in (0, 1):
        folded = jnp.where(low, tiles[d][: per // 2], pltpu.roll(tiles[d][per // 2 :], HALF_LANES, axis=1))
        met[d][0] = folded.astype(BF16)
    own_block(1)
    for d in (0, 1):
        meta_copy(d, 0).start()
        key_row, key_col = keys[d]
        place_col = jnp.sum(ones_where(key_row > key_col), axis=1, keepdims=True)
        for c in range(tok_dev // big):
            back[d][c] = ones_where(place_col == fiota((tok_dev, big), 1) + c * big).astype(BF16)

    def pick_rows(id_col, weight_col, block, slot, store_back, rows):
        scale[slot_rows(slot), :] = weight_col
        gather = ones_where(id_col == fiota((per, rows), 1)).astype(BF16)
        x[t, slot_rows(slot), :] = dot(gather, block).astype(BF16)
        row_copy(slot, t).start()
        square = iota((per, per), 0) == iota((per, per), 1)
        id_row = jnp.sum(jnp.where(square, id_col, 0.0), axis=0, keepdims=True)
        store_back(ones_where(fiota((rows, per), 0) == id_row).astype(BF16))

    def own_rows():
        id_col = jnp.sum(jnp.where(lane_e == z, ids_t, 0.0), axis=1, keepdims=True)
        weight_col = jnp.sum(jnp.where(meta_lane == z + n, weights_t, 0.0), axis=1, keepdims=True)

        def store(value):
            pw_own[...] = value

        pick_rows(id_col, weight_col, tok[...], 0, store, tok_dev)

    def arrived_rows(d, k, rows):
        tile = met[d][k].astype(F32)
        lane = iota((per // 2, LANES), 1)

        def column(at):
            parts = [
                jnp.sum(jnp.where(lane == at + part, tile, 0.0), axis=1, keepdims=True)
                for part in (0, HALF_LANES)
            ]
            return jnp.concatenate(parts, axis=0)

        def store(value):
            pw[d][k, :rows] = value

        slot = slot_of(d, k)
        if not isinstance(k, int):
            pass
        elif k == hops:
            slot = n - 1
        pick_rows(column(z), column(z + n), buf[d][k, :rows], slot, store, rows)

    def token_step(part, q, m, both=True):
        pairs = ((0, q), (1, q - 1)) if both else ((0, q),)
        onward = pieces(m - 1, part)
        for c in pieces(m, part):
            for d, k in pairs:
                token_arrival(d, k, c).wait_recv()
                if c in onward:
                    token_copy(d, k, c).start()
        if part == 0:
            for d, k in pairs:
                meta_arrival(d, k).wait_recv()
                if m > 1:
                    meta_copy(d, k).start()
        if part == (0 if m <= dense // 2 else 1):
            for d, k in pairs:
                arrived_rows(d, k, rows_of(m))

    fc = min(ff, 256)

    def feed_forward(i, first, last):
        r0, rows = first * per, (last - first) * per

        @pl.loop(first, last)
        def _(slot):
            row_copy(slot, 1 - t).wait_recv()

        at = pl.ds(r0, rows)
        hidden = []
        for f in range(0, ff, fc):
            cols = pl.ds(f, fc)
            gate = dot(x[0, at, :], wg[:dh, cols]) + dot(x[1, at, :], wg[dh:, cols])
            up = dot(x[0, at, :], wu[:dh, cols]) + dot(x[1, at, :], wu[dh:, cols])
            hidden.append((gate / (1.0 + jnp.exp(-gate)) * up * scale[at, :]).astype(BF16))
        hidden = jnp.concatenate(hidden, axis=1)
        pout[at, :] = dot(hidden, wd[:, its_half]).astype(BF16)
        part_copy(i, r0, rows).start()
        res[at, :] = dot(hidden, wd[:, my_half]).astype(BF16)

    def join_halves(i, first, last):
        r0, rows = first * per, (last - first) * per
        at = pl.ds(r0, rows)
        part_copy(i, r0, rows).wait_recv()
        res[at, :] = (res[at, :].astype(F32) + pin[at, :].astype(F32)).astype(BF16)

    def add_to(d, k, slot, at):
        return dot(pw[d][k, at], res[slot_rows(slot), :])

    def sum_step(q, m, directions=(0, 1)):
        pairs = [(d, q - d) for d in directions]
        rows_out, n_out = chunks(m)
        rows_in, n_in = chunks(m - 1)
        each = rows_out // rows_in
        order = [n_out - 1] + list(range(n_out - 1)) if m <= dense else list(range(n_out))
        for c in order:
            for d, k in pairs:
                slot = slot_of(d, k)
                if isinstance(k, int) and k == hops:
                    slot = n - 1
                at = span(c, rows_out)
                value = add_to(d, k, slot, at)
                if c * each < n_in:
                    for piece in range(c * each, (c + 1) * each):
                        sum_arrival(d, k, piece, rows_in).wait_recv()
                    value = value + acc[d][k, at].astype(F32)
                acc[d][k, at] = value.astype(BF16)
                sum_copy(d, k, c, rows_out).start()

    def experts_left(q):
        return hops + 1 - q

    bounds = [0, hops // 2 - 1, hops - 1, 5 * hops // 4 + 1, 3 * hops // 2 + 1, n]

    def some_experts(i):
        feed_forward(i, bounds[i], bounds[i + 1])

    def join(i):
        join_halves(i, bounds[i], bounds[i + 1])

    def tokens_of(part, q):
        token_step(part, q, experts_left(q), q > 1)

    def sums_of(q):
        sum_step(q, experts_left(q))

    own_rows()
    for copy in loads[1:]:
        copy.wait()
    full = hops - dense // 2
    alone = full - 2
    token_step(0, 1, hops, False)

    @pl.loop(2, alone + 1)
    def _(q):
        token_step(0, q, hops, True)

    send_own_block(1)
    near = 1
    for q in range(alone + 1, hops + 1):
        tokens_of(0, q)
        tokens_of(1, near)
        if near == hops // 4 + 1:
            some_experts(0)
        near += 1
    some_experts(4)
    tokens_of(1, near)
    join(0)
    join(4)
    for q in range(near + 1, hops - dense + 1):
        tokens_of(1, q)
    tokens_of(1, hops - dense + 1)
    back_hop = hops
    for q in range(hops - dense + 2, full + 1):
        sums_of(back_hop)
        back_hop -= 1
        if q == hops - dense + 2:
            some_experts(1)
        tokens_of(1, q)
        if q == full - 1:
            join(1)
            some_experts(2)
    some_experts(3)
    sum_step(back_hop, experts_left(back_hop), (0,))
    join(2)
    join(3)
    sum_step(back_hop, experts_left(back_hop), (1,))
    back_hop -= 1
    while experts_left(back_hop) <= dense + 1:
        sums_of(back_hop)
        back_hop -= 1
    rest = back_hop

    @pl.loop(0, rest - 1)
    def _(i):
        sum_step(rest - i, hops)

    sum_step(1, hops, (0,))

    for d in (0, 1):
        for k in range(hops - d):
            m = hops - k - d
            rows, count = chunks(m)
            for c in range(min(m, dense)):
                token_copy(d, k, c).wait_send()
            for c in range(count):
                sum_copy(d, k + 1, c, rows).wait_send()
            meta_copy(d, k).wait_send()

    @pl.loop(0, n)
    def _(slot):
        row_copy(slot, t).wait_send()

    for i in range(5):
        part_copy(i, bounds[i] * per, (bounds[i + 1] - bounds[i]) * per).wait_send()

    total = dot(pw_own[...], res[slot_rows(0), :])
    for d in (1, 0):
        for c in range(tok_dev // big):
            sum_arrival(d, 0, c, big).wait_recv()
            total = total + dot(back[d][c], acc[d][0, span(c, big)])
    out_ref[...] = total.astype(BF16)


def per_device(tokens, picks, route_weights, gate_weight, up_weight, down_weight):
    n = lax.axis_size("ep")
    tok_dev, width = tokens.shape
    per = picks.shape[1]
    ff = down_weight.shape[1]
    dh = width // lax.axis_size("tp")
    hops = n // 2
    most = tok_dev // per
    dma = pltpu.SemaphoreType.DMA
    vmem = pltpu.VMEM
    kernel = pl.pallas_call(
        functools.partial(kernel_body, n, tok_dev, per, dh, ff),
        out_shape=jax.ShapeDtypeStruct((tok_dev, dh), BF16),
        in_specs=[
            pl.BlockSpec(memory_space=pl.ANY),
            pl.BlockSpec(memory_space=vmem),
            pl.BlockSpec(memory_space=vmem),
            pl.BlockSpec(memory_space=pl.ANY),
            pl.BlockSpec(memory_space=pl.ANY),
            pl.BlockSpec(memory_space=pl.ANY),
        ],
        out_specs=pl.BlockSpec(memory_space=vmem),
        scratch_shapes=[
            vmem((tok_dev, dh), BF16),
            vmem((width, ff), BF16),
            vmem((width, ff), BF16),
            vmem((ff, width), BF16),
            vmem((hops + 1, tok_dev, dh), BF16),
            vmem((hops, tok_dev, dh), BF16),
            vmem((hops + 1, per // 2, LANES), BF16),
            vmem((hops, per // 2, LANES), BF16),
            vmem((hops + 1, tok_dev, dh), BF16),
            vmem((hops, tok_dev, dh), BF16),
            vmem((2, n * per, dh), BF16),
            vmem((n * per, dh), BF16),
            vmem((n * per, dh), BF16),
            vmem((n * per, dh), BF16),
            vmem((hops + 1, tok_dev, per), BF16),
            vmem((hops, tok_dev, per), BF16),
            vmem((tok_dev, per), BF16),
            vmem((n * per, 1), F32),
            vmem((tok_dev // (2 * per), tok_dev, 2 * per), BF16),
            vmem((tok_dev // (2 * per), tok_dev, 2 * per), BF16),
            dma((4,)),
            dma((hops + 1, most)), dma((hops + 1, most)), dma((hops, most)), dma((hops, most)),
            dma((2, hops + 1)), dma((2, hops + 1)),
            dma((n,)), dma((n,)),
            dma((5,)), dma((5,)),
            dma((hops + 1, most)), dma((hops + 1, most)), dma((hops, most)), dma((hops, most)),
        ],
        compiler_params=pltpu.CompilerParams(
            collective_id=0, has_side_effects=True, vmem_limit_bytes=67043328
        ),
    )
    return kernel(tokens, picks, route_weights, gate_weight, up_weight, down_weight)


def solution(mesh):
    return jax.shard_map(
        per_device,
        mesh=mesh,
        in_specs=(
            P(("grp", "ep"), None),
            P(None, ("grp", "ep")),
            P(None, ("grp", "ep")),
            P("ep", None, "tp"),
            P("ep", None, "tp"),
            P("ep", "tp", None),
        ),
        out_specs=P(("grp", "ep"), "tp"),
        check_vma=False,
    )
```
